256 devices in a mesh: ep: 64 (over z, x, core), tp: 4 (over y).
Axes of the slice: x: 4, y: 4, z: 8, core: 2. Of those that a mesh axis runs over, the one named last changes fastest.
Arguments:
- mix_bgate: bfloat16 [16384, 1024], P('ep', 'tp'), may hold values from -6 to 6
- mix_cgate: bfloat16 [16384, 1024], P('ep', 'tp'), may hold values from -6 to 6
- mix_input: bfloat16 [16384, 1024], P('ep', 'tp'), may hold values from -6 to 6
- conv_taps: float32 [3, 1024], P(None, 'tp'), may hold values from -3.5 to 3.5
- mix_out_w: bfloat16 [1024, 2048], P('tp'), may hold values from -0.1875 to 0.1875
- moe_x: bfloat16 [16384, 2048], P('ep', 'tp'), may hold values from -6 to 6
- moe_gain: float32 [2048], replicated, may hold values from 0.1 to 1.9
- routes: int32 [16384, 2], P('ep'), may hold values from 0 to 63, all different within a row; in each aligned block of 256 rows (0 to 255, 256 to 511, ...) at most 12 rows name the same one
- route_w: float32 [16384, 2], P('ep'), may hold values from 0.2 to 1
- w_gate: bfloat16 [64, 2048, 3584], P('ep', None, 'tp'), may hold values from -0.125 to 0.125
- w_up: bfloat16 [64, 2048, 3584], P('ep', None, 'tp'), may hold values from -0.125 to 0.125
- w_down: bfloat16 [64, 3584, 2048], P('ep', 'tp'), may hold values from -0.09375 to 0.09375
Outputs:
- mixed: bfloat16 [16384, 2048], P(('ep', 'tp'))
- routed: bfloat16 [16384, 2048], P('ep', 'tp')
The draws below stay inside these ranges and needn't reach their ends.
Inputs may be any that keep to these rules, and one draw needn't show every extreme that they name: `routes`: among the 256 rows of one index of ep, each row names 2 different experts and no expert is named by more than 12 rows; in every draw some expert is named by exactly 12 rows of some index.
All inputs are finite; a program needn't handle non-finite values.
Results may differ from the reference program's by a relative error of at most 0.012.
Values may be sent and summed in bfloat16 or wider, within the bound.
A program may use at most 64 MiB of HBM per device.

```python
import math
import jax
import jax.numpy as jnp
import numpy as np
from jax import lax

D = 2048
CONV = 1024
TAPS = 3
FF_E = 3584
TOPK = 2
TOK_MOE = 256
SEQ = 16384
MOE_TOKENS = 16384
EXPERTS = 64
CAP = 12
N_EP = 64
N_TP = 4


def steps_of(stream_key, shape, split, low, top_value):
    def one(position, shards_of):
        steps = jax.random.uniform(jax.random.fold_in(jax.random.fold_in(stream_key, 6), position), (shards_of,), jnp.float32, low / len(split), top_value / len(split))
        return jnp.repeat(jnp.exp(steps), shape[position] // shards_of).reshape((-1,) + (1,) * (len(shape) - position - 1))

    loudness = one(*split[0])
    for cut in split[1:]:
        loudness = loudness * one(*cut)
    return loudness


def assign_block(own_key, own, number, rows, amount, top, bound, skew):
    sequence = jax.random.permutation(own_key, amount)
    heavy_load, ordinary = portions_of(amount, rows * top, bound, skew, True), portions_of(amount, rows * top, bound, skew, False)
    places = jnp.arange(amount)

    def named(lengths, offset_by):
        used = int((lengths > 0).sum())
        fixed = max(1, used // 4)
        moved = fixed + (places - fixed + offset_by * (used - fixed)) % max(1, amount - fixed)
        return jnp.zeros((amount,), jnp.int32).at[sequence[jnp.where(places < fixed, places, moved)]].set(jnp.asarray(lengths, jnp.int32))

    lengths = jnp.where(number % 4 == 0, named(heavy_load, number // 4), named(ordinary, number - number // 4 - 1))
    mixed = jax.random.permutation(jax.random.fold_in(own, 3), amount)
    source_of, taker = mixed[0:amount // 2 * 2:2], mixed[1:amount // 2 * 2:2]
    slack = jnp.minimum(lengths[source_of] - 1, bound - lengths[taker]) // 2
    slack = jnp.where((source_of == sequence[0]) | (taker == sequence[0]) | (lengths[taker] == 0), 0, jnp.maximum(slack, 0))
    moved = jax.random.randint(jax.random.fold_in(own, 4), (amount // 2,), 0, 1 << 20) % (slack + 1)
    lengths = lengths.at[source_of].add(-moved).at[taker].add(moved)
    items = jnp.searchsorted(jnp.cumsum(lengths), jnp.arange(rows * top), side="right").astype(jnp.int32)
    listing = items.reshape(top, rows).T
    listing = listing[jax.random.permutation(jax.random.fold_in(own, 1), rows)]
    offset_by = jax.random.randint(jax.random.fold_in(own, 2), (rows, 1), 0, top)
    return jnp.take_along_axis(listing, (jnp.arange(top)[None, :] + offset_by) % top, axis=1)


def portions_of(amount, total, reach, lean, full):
    loads = [(1 << 20) // math.isqrt(grade ** lean) + 1 for grade in range(1, amount + 1)]
    largest = reach if full else min(reach, max(-(-total // amount), total * loads[0] // sum(loads)))
    least = 1 if total - largest >= amount - 1 else 0
    counts, surplus = [largest] + [least] * (amount - 1), total - largest - least * (amount - 1)
    while surplus > 0:
        candidates = [i for i in range(1, amount) if counts[i] < largest] or [i for i in range(1, amount) if counts[i] < reach]
        pool, budget = sum([loads[i] for i in candidates]), surplus
        for i in candidates:
            more = min(reach - counts[i], max(1, budget * loads[i] // pool), surplus)
            counts[i] = counts[i] + more
            surplus = surplus - more
    return np.array(counts)


def normal_values(rng, extent, spread, reach, shards=(), kind=jnp.bfloat16):
    factor_of = steps_of(rng, extent, shards, -0.22, 0.18) if shards else 1.0
    array = jax.random.normal(rng, extent, jnp.float32) * spread * factor_of
    return jnp.minimum(jnp.maximum(array, -reach), reach).astype(kind)


def setup_inputs(seed: int = 0) -> dict:
    key_of = jax.random.split(jax.random.key(seed), 13)
    mix_bgate = normal_values(key_of[0], (SEQ, CONV), 1.0, 6.0, ((0, 64), (1, 4)))
    mix_cgate = normal_values(key_of[1], (SEQ, CONV), 1.0, 6.0, ((0, 64), (1, 4)))
    mix_input = normal_values(key_of[2], (SEQ, CONV), 1.0, 6.0, ((0, 64), (1, 4)))
    conv_taps = normal_values(key_of[3], (TAPS, CONV), TAPS ** -0.5, 3.5, ((1, 4),), jnp.float32)
    mix_out_w = normal_values(key_of[4], (CONV, D), CONV ** -0.5, 0.1875, ((0, 4),))
    moe_x = normal_values(key_of[5], (MOE_TOKENS, D), 1.0, 6.0, ((0, 64), (1, 4)))
    moe_gain = jnp.clip(1.0 + 0.18 * jax.random.normal(key_of[6], (D,), jnp.float32), 0.1, 1.9)
    routes_keys = jax.random.split(jax.random.fold_in(key_of[7], 1), MOE_TOKENS // TOK_MOE)
    routes_turns = jax.random.permutation(jax.random.fold_in(key_of[7], 3), MOE_TOKENS // TOK_MOE)
    routes = jax.vmap(lambda own, number: assign_block(jax.random.fold_in(key_of[7], 2), own, number, TOK_MOE, EXPERTS, TOPK, CAP, 2))(routes_keys, routes_turns).reshape((MOE_TOKENS, TOPK))
    route_w = jnp.clip(0.2 + 0.8 * jax.random.uniform(key_of[8], (MOE_TOKENS, TOPK), jnp.float32) ** steps_of(key_of[8], (MOE_TOKENS, TOPK), ((0, 64),), -0.2, 0.2), 0.2, 1.0)
    w_gate = normal_values(key_of[9], (EXPERTS, D, FF_E), D ** -0.5, 0.125, ((0, 64), (2, 4)))
    w_up = normal_values(key_of[10], (EXPERTS, D, FF_E), D ** -0.5, 0.125, ((0, 64), (2, 4)))
    w_down = normal_values(key_of[11], (EXPERTS, FF_E, D), FF_E ** -0.5, 0.09375, ((0, 64), (1, 4)))
    return {"mix_bgate": mix_bgate, "mix_cgate": mix_cgate, "mix_input": mix_input, "conv_taps": conv_taps, "mix_out_w": mix_out_w, "moe_x": moe_x, "moe_gain": moe_gain, "routes": routes, "route_w": route_w, "w_gate": w_gate, "w_up": w_up, "w_down": w_down}


def rms_rows(values, gain):
    wide = values.astype(jnp.float32)
    scale = lax.rsqrt(lax.optimization_barrier(jnp.mean(wide * wide, axis=-1, keepdims=True)) + 1e-06)
    return (wide * scale * gain).astype(jnp.bfloat16)

def rounded(value):
    return lax.optimization_barrier(value.astype(jnp.bfloat16)).astype(jnp.float32)

def reference(mix_bgate, mix_cgate, mix_input, conv_taps, mix_out_w, moe_x, moe_gain, routes, route_w, w_gate, w_up, w_down):
    length = mix_input.shape[0]
    prod = mix_cgate.astype(jnp.float32) * mix_input.astype(jnp.float32)
    padded = jnp.pad(prod, ((TAPS - 1, 0), (0, 0)))
    conv = conv_taps[0] * padded[0:length]
    for j in range(1, TAPS):
        conv = conv + conv_taps[j] * padded[j:j + length]
    gated = (mix_bgate.astype(jnp.float32) * conv).astype(jnp.bfloat16)
    step = CONV // N_TP
    total = jnp.zeros((length, D), jnp.float32)
    for q in range(N_TP):
        part = jnp.dot(gated[:, q * step:(q + 1) * step], mix_out_w[q * step:(q + 1) * step], preferred_element_type=jnp.float32)
        total = total + rounded(part)
    mixed = total.astype(jnp.bfloat16)
    normed = rms_rows(moe_x, moe_gain)
    dev_routes = routes.reshape(N_EP, TOK_MOE * TOPK)
    onehot = (dev_routes[:, :, None] == jnp.arange(EXPERTS, dtype=jnp.int32)[None, None, :]).astype(jnp.int32)
    earlier = jnp.cumsum(onehot, axis=1) - onehot
    slot = lax.optimization_barrier(jnp.sum(earlier * onehot, axis=2))
    row = jnp.arange(N_EP, dtype=jnp.int32)[:, None] * CAP + slot
    flat_e = dev_routes.reshape(-1)
    flat_row = row.reshape(-1).astype(jnp.int32)
    token = jnp.arange(MOE_TOKENS * TOPK, dtype=jnp.int32) // TOPK
    buffers = jnp.zeros((EXPERTS, N_EP * CAP, D), jnp.bfloat16).at[flat_e, flat_row].set(normed[token])
    fstep = FF_E // N_TP

    def expert(items):
        rows, wg, wu, wd = items
        gate = jnp.dot(rows, wg, preferred_element_type=jnp.float32)
        upper = jnp.dot(rows, wu, preferred_element_type=jnp.float32)
        hidden = (jax.nn.silu(gate) * upper).astype(jnp.bfloat16)
        acc = jnp.zeros((rows.shape[0], D), jnp.float32)
        for q in range(N_TP):
            part = jnp.dot(hidden[:, q * fstep:(q + 1) * fstep], wd[q * fstep:(q + 1) * fstep], preferred_element_type=jnp.float32)
            acc = acc + rounded(part)
        return acc.astype(jnp.bfloat16)
    results = lax.map(expert, (buffers, w_gate, w_up, w_down))
    picked = results[flat_e, flat_row].astype(jnp.float32).reshape(MOE_TOKENS, TOPK, D)
    routed = lax.optimization_barrier(jnp.sum(picked * route_w[:, :, None], axis=1)).astype(jnp.bfloat16)
    return (mixed, routed)
```

```python
import functools

import jax
import jax.numpy as jnp
from jax import lax
from jax.experimental import pallas as pl
from jax.experimental.pallas import tpu as pltpu
from jax.sharding import PartitionSpec as P

CAP = 12
TP = 4
BF = jnp.bfloat16
F32 = jnp.float32


def iota(shape, dim):
    return lax.broadcasted_iota(jnp.int32, shape, dim)


def to_message(v, groups):
    h = v.shape[1] // 2
    v0 = v[:, :h].reshape(groups // 2, 8, h)
    v1 = v[:, h:].reshape(groups // 2, 8, h)
    low = iota(v0.shape, 1) < 4
    even = jnp.where(low, v0, pltpu.roll(v1, 4, axis=1))
    odd = jnp.where(low, pltpu.roll(v0, 4, axis=1), v1)
    return even, odd


def from_message(m, groups):
    h = m.shape[2]
    pairs = m.reshape(groups // 2, 2, 8, h)
    even, odd = pairs[:, 0], pairs[:, 1]
    low = iota(even.shape, 1) < 4
    v0 = jnp.where(low, even, pltpu.roll(odd, 4, axis=1))
    v1 = jnp.where(low, pltpu.roll(even, 4, axis=1), odd)
    return v0.reshape(groups * 4, h), v1.reshape(groups * 4, h)


def kernel(
    dims,
    bg, cg, ci, taps, mixw, x, gain, routes, rw, wg, wu, wd,
    mixed, routed,
    wg_v, wu_v, wd_v, mw_v, out, G, nrm, PS, R1, FR, ACC, FIN, ret,
    halo, MS, MR1, MF, MACC,
    wsem, halo_s, halo_r, disp_s, disp_r, gd_s, gd_r, gr_s, gr_r,
    r1_s, r1_r, fi_s, fi_r, fa_s, fa_r, back_s, back_r,
    m1_s, m1_r, mi_s, mi_r, ma_s, ma_r,
):
    NZ, NX, order = dims
    S = NX * 2
    H = S // 2
    n_ep = NZ * S
    ntok, DS = x.shape
    h = DS // 2
    rows = S * CAP
    ar = S * 8
    i = lax.axis_index("ep")
    y = lax.axis_index("tp")
    up = lax.rem(y + 1, TP)
    down = lax.rem(y + 3, TP)
    far = lax.rem(y + 2, TP)
    iz, ix, ic = i // S, (i % S) // 2, i % 2
    sides = ((0, up), (1, down))

    def dz_of(c):
        dz = jnp.int32(0)
        for n in range(NZ):
            dz = jnp.where(c == n, order[n], dz)
        return dz

    def target(c, r):
        return (((iz + dz_of(c)) % NZ) * NX + (ix + r // 2) % NX) * 2 + (ic + r % 2) % 2

    def source(c, r):
        return (((iz + NZ - dz_of(c)) % NZ) * NX + (ix + NX - r // 2) % NX) * 2 + (ic + r % 2) % 2

    def remote(src, dst, ssem, rsem, ep=None, tp=None):
        return pltpu.make_async_remote_copy(
            src_ref=src, dst_ref=dst, send_sem=ssem, recv_sem=rsem,
            device_id=(i if ep is None else ep, y if tp is None else tp),
            device_id_type=pl.DeviceIdType.MESH,
        )

    def arrived(ref, sem):
        remote(ref, ref, sem, sem, tp=up).wait_recv()

    def left(ref, sem):
        remote(ref, ref, sem, sem, tp=up).wait_send()

    barrier = pltpu.get_barrier_semaphore()

    @pl.loop(1, n_ep)
    def _(d):
        pl.semaphore_signal(
            barrier, inc=1, device_id=(lax.rem(i + d, n_ep), y), device_id_type=pl.DeviceIdType.MESH
        )

    for _, other in sides:
        pl.semaphore_signal(barrier, inc=1, device_id=(i, other), device_id_type=pl.DeviceIdType.MESH)

    loads = [
        pltpu.make_async_copy(mixw, mw_v, wsem.at[0]),
        pltpu.make_async_copy(wg.at[0], wg_v, wsem.at[1]),
        pltpu.make_async_copy(wu.at[0], wu_v, wsem.at[2]),
        pltpu.make_async_copy(wd.at[0], wd_v, wsem.at[3]),
    ]
    for load in loads:
        load.start()

    e = routes[...]
    dz = (e // S + NZ - iz) & (NZ - 1)
    chunk = jnp.zeros_like(e)
    for n in range(NZ):
        chunk = jnp.where(dz == order[n], n, chunk)
    er = e & (S - 1)
    dx = ((er // 2) + NX - ix) & (NX - 1)
    dc = (er + ic) & 1
    k = chunk * S + dx * 2 + dc
    hot = [iota((n_ep, ntok), 0) == k[q : q + 1] for q in range(2)]
    named = jnp.where(hot[0] | hot[1], 1.0, 0.0).astype(BF)
    before = jnp.where(iota((ntok, ntok), 0) < iota((ntok, ntok), 1), 1.0, 0.0).astype(BF)
    rank = jnp.dot(named, before, preferred_element_type=F32)
    marks = []
    for q in range(2):
        slot = jnp.sum(jnp.where(hot[q], rank, 0.0), axis=0, keepdims=True).astype(jnp.int32)
        kq = k[q : q + 1]
        marks.append(
            (jnp.where(slot < 8, kq * 8 + slot, -1), jnp.where(slot >= 8, kq * 4 + slot - 8, -1))
        )
    ia = iota((n_ep * 8, ntok), 0)
    ib = iota((n_ep * 4, ntok), 0)
    pa = jnp.where((ia == marks[0][0]) | (ia == marks[1][0]), 1.0, 0.0).astype(BF)
    pb = jnp.where((ib == marks[0][1]) | (ib == marks[1][1]), 1.0, 0.0).astype(BF)
    xv = x[...]
    oa = jnp.dot(pa, xv, preferred_element_type=F32).reshape(n_ep, 8, DS).astype(BF)
    out[:, :, :DS] = oa
    even, odd = to_message(jnp.dot(pb, xv, preferred_element_type=F32), n_ep)
    for p in range(n_ep // 2):
        out[2 * p, :, DS:] = even[p].astype(BF)
        out[2 * p + 1, :, DS:] = odd[p].astype(BF)
    G[0, 0, 0] = out[0]

    pl.semaphore_wait(barrier, n_ep - 1 + 2)

    nxt = lax.rem(i + 1, n_ep)
    ntail = cg.shape[0] - 8
    tails = [
        remote(ref.at[pl.ds(ntail, 8)], halo.at[q], halo_s.at[q], halo_r.at[q], ep=nxt)
        for q, ref in enumerate((cg, ci))
    ]
    for tail in tails:
        tail.start()

    @pl.loop(1, n_ep)
    def _(kk):
        c, r = kk // S, kk % S
        remote(out.at[kk], G.at[0, c, r], disp_s, disp_r.at[c], ep=target(c, r)).start()

    loads[0].wait()
    for tail in tails:
        tail.wait_recv()
    prev = halo[0].astype(F32) * halo[1].astype(F32)
    prev = jnp.where(i > 0, prev, 0.0)
    prod = cg[...].astype(F32) * ci[...].astype(F32)
    row = iota(prod.shape, 0)
    back1 = jnp.where(row == 0, prev[7:8], pltpu.roll(prod, 1, axis=0))
    back2 = jnp.where(row == 0, prev[6:7], jnp.where(row == 1, prev[7:8], pltpu.roll(prod, 2, axis=0)))
    tv = taps[...]
    conv = tv[0:1] * back2 + tv[1:2] * back1 + tv[2:3] * prod
    gated = (bg[...].astype(F32) * conv).astype(BF)
    mrows = MS.shape[1]
    mh = mrows // 2
    for q in range(TP):
        MS[q] = jnp.dot(
            gated[q * mrows : (q + 1) * mrows], mw_v[...], preferred_element_type=F32
        ).astype(BF)
    for d, other in sides:
        remote(
            MS.at[far, pl.ds(d * mh, mh)], MR1.at[d], m1_s.at[d], m1_r.at[d], tp=other
        ).start()
        keep = (1 - d) * mh
        remote(
            MS.at[other, pl.ds(keep, mh)], MF.at[d, pl.ds(keep, mh)], mi_s.at[d], mi_r.at[d], tp=other
        ).start()

    def stage_direct(c):
        @pl.when(c == 0)
        def _():
            arrived(G.at[0, 0, pl.ds(1, S - 1)], disp_r.at[0])

        @pl.when(c > 0)
        def _():
            arrived(G.at[0, c], disp_r.at[c])

        for d, other in sides:
            remote(G.at[0, c], G.at[1 + d, c], gd_s.at[d], gd_r.at[d, c], tp=other).start()

    def stage_relay(c):
        for d, other in sides:
            arrived(G.at[1 + d, c], gd_r.at[d, c])
            half = pl.ds(d * H, H)
            remote(G.at[1 + d, c, half], G.at[3, c, half], gr_s.at[d], gr_r.at[d, c], tp=other).start()

    def stage_expert(c):
        for d in range(2):
            arrived(G.at[3, c, pl.ds(d * H, H)], gr_r.at[d, c])
        owners = (y, down, up, far)
        total = jnp.zeros((S, 8, 1), F32)
        total_b = jnp.zeros((S, 8, 1), F32)
        for n in range(TP):
            g = G[n, c].astype(F32)
            a, b = g[:, :, :DS], g[:, :, DS:]
            total = total + jnp.sum(a * a, axis=2, keepdims=True)
            total_b = total_b + jnp.sum(b * b, axis=2, keepdims=True)
        width = DS * TP
        total_b = total_b + pltpu.roll(total_b, 4, axis=1)
        sa = lax.rsqrt(total / width + 1e-06)
        sb = lax.rsqrt(total_b / width + 1e-06)
        for n, owner in enumerate(owners):
            g = G[n, c].astype(F32)
            gn = gain[owner]
            nrm[owner, pl.ds(0, ar), :] = (g[:, :, :DS] * sa).reshape(ar, DS).astype(F32) * gn
            v0, v1 = from_message(g[:, :, DS:] * sb, S)
            nrm[owner, pl.ds(ar, rows - ar), pl.ds(0, h)] = v0 * gn[:, :h]
            nrm[owner, pl.ds(ar, rows - ar), pl.ds(h, h)] = v1 * gn[:, h:]
        lhs = jnp.concatenate([nrm[n].astype(BF) for n in range(TP)], axis=1)
        gate = jnp.dot(lhs, wg_v[...], preferred_element_type=F32)
        upper = jnp.dot(lhs, wu_v[...], preferred_element_type=F32)
        hidden = (gate / (1.0 + jnp.exp(-gate)) * upper).astype(BF)
        for q in range(TP):
            part = jnp.dot(hidden, wd_v[:, q * DS : (q + 1) * DS], preferred_element_type=F32)
            PS[c, q, :, :, pl.ds(0, DS)] = part[:ar].reshape(S, 8, DS).astype(BF)
            even, odd = to_message(part[ar:], S)
            for p in range(H):
                PS[c, q, 2 * p, :, pl.ds(DS, h)] = even[p].astype(BF)
                PS[c, q, 2 * p + 1, :, pl.ds(DS, h)] = odd[p].astype(BF)
        for d, other in sides:
            half, rest = pl.ds(d * H, H), pl.ds((1 - d) * H, H)
            remote(PS.at[c, far, half], R1.at[d, c], r1_s.at[d], r1_r.at[d, c], tp=other).start()
            remote(PS.at[c, other, rest], FR.at[d, c, rest], fi_s.at[d], fi_r.at[d, c], tp=other).start()

    def stage_add(c):
        for d, other in sides:
            half = pl.ds(d * H, H)
            arrived(R1.at[d, c], r1_r.at[d, c])
            ACC[d, c] = (PS[c, other, half].astype(F32) + R1[d, c].astype(F32)).astype(BF)
            remote(ACC.at[d, c], FR.at[d, c, half], fa_s.at[d], fa_r.at[d, c], tp=other).start()

    def stage_back(c):
        for d in range(2):
            arrived(FR.at[d, c, pl.ds((1 - d) * H, H)], fi_r.at[d, c])
            arrived(FR.at[d, c, pl.ds(d * H, H)], fa_r.at[d, c])
        whole = PS[c, y].astype(F32) + FR[0, c].astype(F32) + FR[1, c].astype(F32)
        FIN[c] = whole.astype(BF)

        @pl.when(c == 0)
        def _():
            ret[0, 0] = FIN[0, 0]

        @pl.loop(0, S)
        def _(r):
            @pl.when(c + r > 0)
            def _():
                remote(FIN.at[c, r], ret.at[c, r], back_s, back_r.at[c], ep=source(c, r)).start()

    for load in loads[1:]:
        load.wait()

    @pl.loop(0, NZ + 4)
    def _(t):
        @pl.when(t < NZ)
        def _():
            stage_direct(t)

        @pl.when((t >= 1) & (t < NZ + 1))
        def _():
            stage_relay(t - 1)

        @pl.when((t >= 3) & (t < NZ + 3))
        def _():
            stage_add(t - 3)

        @pl.when(t >= 4)
        def _():
            stage_back(t - 4)

        @pl.when((t >= 2) & (t < NZ + 2))
        def _():
            stage_expert(t - 2)

        @pl.when(t == NZ)
        def _():
            for d, other in sides:
                half = pl.ds(d * mh, mh)
                arrived(MR1.at[d], m1_r.at[d])
                MACC[d] = (MS[other, half].astype(F32) + MR1[d].astype(F32)).astype(BF)
                remote(MACC.at[d], MF.at[d, half], ma_s.at[d], ma_r.at[d], tp=other).start()

    for d in range(2):
        arrived(MF.at[d, pl.ds((1 - d) * mh, mh)], mi_r.at[d])
        arrived(MF.at[d, pl.ds(d * mh, mh)], ma_r.at[d])
    mixed[...] = (MS[y].astype(F32) + MF[0].astype(F32) + MF[1].astype(F32)).astype(BF)

    table = jnp.concatenate(
        [marks[0][0].astype(F32), marks[1][0].astype(F32), marks[0][1].astype(F32), marks[1][1].astype(F32), rw[...]]
        + [jnp.zeros((122, ntok), F32)],
        axis=0,
    )
    cols = jnp.transpose(table)
    ga = iota((ntok, n_ep * 8), 1)
    gb = iota((ntok, n_ep * 4), 1)
    pick = []
    for q in range(2):
        pick.append(
            (
                jnp.where(ga == cols[:, q : q + 1].astype(jnp.int32), 1.0, 0.0).astype(BF),
                jnp.where(gb == cols[:, 2 + q : 3 + q].astype(jnp.int32), 1.0, 0.0).astype(BF),
                cols[:, 4 + q : 5 + q],
            )
        )
    arrived(ret.at[0, pl.ds(1, S - 1)], back_r.at[0])
    for c in range(1, NZ):
        arrived(ret.at[c], back_r.at[c])
    back = ret[...].reshape(n_ep, 8, DS + h)
    ra = back[:, :, :DS].reshape(n_ep * 8, DS)
    b0, b1 = from_message(back[:, :, DS:].astype(F32), n_ep)
    rb = jnp.concatenate([b0, b1], axis=1).astype(BF)
    total = jnp.zeros((ntok, DS), F32)
    for q in range(2):
        row = jnp.dot(pick[q][0], ra, preferred_element_type=F32)
        row = row + jnp.dot(pick[q][1], rb, preferred_element_type=F32)
        total = total + row * pick[q][2]
    routed[...] = total.astype(BF)

    for tail in tails:
        tail.wait_send()
    left(out.at[pl.ds(1, n_ep - 1)], disp_s)
    left(out.at[pl.ds(1, n_ep - 1)], back_s)
    for d in range(2):
        left(G.at[0], gd_s.at[d])
        left(R1.at[0], gr_s.at[d])
        left(R1.at[0], r1_s.at[d])
        left(R1.at[0], fi_s.at[d])
        left(R1.at[0], fa_s.at[d])
        left(MR1.at[0], m1_s.at[d])
        left(MR1.at[0], mi_s.at[d])
        left(MR1.at[0], ma_s.at[d])


def body(mix_bgate, mix_cgate, mix_input, conv_taps, mix_out_w, moe_x, moe_gain, routes, route_w, w_gate, w_up, w_down, *, dims):
    NZ, NX, order = dims
    S = NX * 2
    H = S // 2
    n_ep = NZ * S
    ntok, DS = moe_x.shape
    D = DS * TP
    F = w_gate.shape[2]
    CH = mix_out_w.shape[0]
    ML = DS + DS // 2
    mrows = mix_input.shape[0] // TP
    vmem = pl.BlockSpec(memory_space=pltpu.VMEM)
    anyspace = pl.BlockSpec(memory_space=pl.ANY)
    V = pltpu.VMEM
    dma = pltpu.SemaphoreType.DMA
    return pl.pallas_call(
        functools.partial(kernel, dims),
        name="step",
        out_shape=(
            jax.ShapeDtypeStruct((mrows, D), BF),
            jax.ShapeDtypeStruct((ntok, DS), BF),
        ),
        in_specs=[vmem, vmem, vmem, vmem, anyspace, vmem, vmem, vmem, vmem, anyspace, anyspace, anyspace],
        out_specs=(vmem, vmem),
        scratch_shapes=[
            V((D, F), BF), V((D, F), BF), V((F, D), BF), V((CH, D), BF),
            V((n_ep, 8, ML), BF),
            V((4, NZ, S, 8, ML), BF),
            V((TP, S * CAP, DS), F32),
            V((NZ, TP, S, 8, ML), BF),
            V((2, NZ, H, 8, ML), BF),
            V((2, NZ, S, 8, ML), BF),
            V((2, NZ, H, 8, ML), BF),
            V((NZ, S, 8, ML), BF),
            V((NZ, S, 8, ML), BF),
            V((2, 8, CH), BF),
            V((TP, mrows, D), BF),
            V((2, mrows // 2, D), BF),
            V((2, mrows, D), BF),
            V((2, mrows // 2, D), BF),
            dma((4,)), dma((2,)), dma((2,)),
            dma, dma((NZ,)),
            dma((2,)), dma((2, NZ)), dma((2,)), dma((2, NZ)),
            dma((2,)), dma((2, NZ)), dma((2,)), dma((2, NZ)), dma((2,)), dma((2, NZ)),
            dma, dma((NZ,)),
            dma((2,)), dma((2,)), dma((2,)), dma((2,)), dma((2,)), dma((2,)),
        ],
        compiler_params=pltpu.CompilerParams(
            collective_id=0, has_side_effects=True, vmem_limit_bytes=60 * 1024 * 1024
        ),
    )(
        mix_bgate, mix_cgate, mix_input, conv_taps, mix_out_w, moe_x,
        moe_gain.reshape(TP, 1, DS), routes.T, route_w.T, w_gate, w_up, w_down,
    )


def solution(mesh):
    n_ep = mesh.shape["ep"]
    NZ, NX = (8, n_ep // 16) if n_ep >= 32 else (2, n_ep // 4)
    order = (0, 2, 6, 3, 5, 4, 1, 7) if NZ == 8 else tuple(range(NZ))
    in_specs = (
        P("ep", "tp"), P("ep", "tp"), P("ep", "tp"), P(None, "tp"), P("tp", None), P("ep", "tp"), P(),
        P("ep", None), P("ep", None), P("ep", None, "tp"), P("ep", None, "tp"), P("ep", "tp", None),
    )
    out_specs = (P(("ep", "tp"), None), P("ep", "tp"))
    return jax.shard_map(
        functools.partial(body, dims=(NZ, NX, order)),
        mesh=mesh, in_specs=in_specs, out_specs=out_specs, check_vma=False,
    )
```

```python
import functools

import jax
import jax.numpy as jnp
from jax import lax
from jax.experimental import pallas as pl
from jax.experimental.pallas import tpu as pltpu
from jax.sharding import PartitionSpec as P

CAP = 12
TP = 4
BF = jnp.bfloat16
F32 = jnp.float32


def iota(shape, dim):
    return lax.broadcasted_iota(jnp.int32, shape, dim)


def to_message(v, groups):
    h = v.shape[1] // 2
    v0 = v[:, :h].reshape(groups // 2, 8, h)
    v1 = v[:, h:].reshape(groups // 2, 8, h)
    low = iota(v0.shape, 1) < 4
    even = jnp.where(low, v0, pltpu.roll(v1, 4, axis=1))
    odd = jnp.where(low, pltpu.roll(v0, 4, axis=1), v1)
    return even, odd


def from_message(m, groups):
    h = m.shape[2]
    pairs = m.reshape(groups // 2, 2, 8, h)
    even, odd = pairs[:, 0], pairs[:, 1]
    low = iota(even.shape, 1) < 4
    v0 = jnp.where(low, even, pltpu.roll(odd, 4, axis=1))
    v1 = jnp.where(low, pltpu.roll(even, 4, axis=1), odd)
    return v0.reshape(groups * 4, h), v1.reshape(groups * 4, h)


def kernel(
    dims,
    bg_h, cg_h, ci_h, taps_h, mixw, x_h, gain_h, routes_h, rw_h, wg, wu, wd,
    mixed, routed,
    bg, cg, ci, taps, x, gain, routes, rw,
    wg_v, wu_v, wd_v, mw_v, out, G, nrm, PS, R1, FR, ACC, FIN, ret,
    halo, MS, MR1, MF, MACC, pick_a, pick_b,
    wsem, halo_s, halo_r, disp_s, disp_r, gd_s, gd_r, gr_s, gr_r,
    r1_s, r1_r, fi_s, fi_r, fa_s, fa_r, back_s, back_r,
    m1_s, m1_r, mi_s, mi_r, ma_s, ma_r,
):
    NZ, NX, order = dims
    S = NX * 2
    H = S // 2
    n_ep = NZ * S
    ntok, DS = x.shape
    h = DS // 2
    rows = S * CAP
    ar = S * 8
    i = lax.axis_index("ep")
    y = lax.axis_index("tp")
    up = (y + 1) & (TP - 1)
    down = (y + 3) & (TP - 1)
    far = (y + 2) & (TP - 1)
    ic = i & 1
    ix = (i >> 1) & (NX - 1)
    iz = i // S
    sides = ((0, up), (1, down))

    def device(dz, dx, dc):
        return ((((iz + dz) & (NZ - 1)) * NX + ((ix + dx) & (NX - 1))) << 1) + ((ic + dc) & 1)

    def dz_of(c):
        dz = jnp.int32(0)
        for n in range(NZ):
            dz = jnp.where(c == n, order[n], dz)
        return dz

    def remote(src, dst, ssem, rsem, ep=None, tp=None):
        return pltpu.make_async_remote_copy(
            src_ref=src, dst_ref=dst, send_sem=ssem, recv_sem=rsem,
            device_id=(i if ep is None else ep, y if tp is None else tp),
            device_id_type=pl.DeviceIdType.MESH,
        )

    def arrived(ref, sem):
        remote(ref, ref, sem, sem, tp=up).wait_recv()

    def left(ref, sem):
        remote(ref, ref, sem, sem, tp=up).wait_send()

    barrier = pltpu.get_barrier_semaphore()

    def greet(ep, tp):
        pl.semaphore_signal(barrier, inc=1, device_id=(ep, tp), device_id_type=pl.DeviceIdType.MESH)

    for dz in sorted(range(NZ), key=lambda n: -min(n, NZ - n)):
        for r in range(S):
            if dz + r:
                greet(device(dz, r // 2, r % 2), y)
    for _, other in sides:
        greet(i, other)

    loads = [
        pltpu.make_async_copy(src, dst, wsem.at[n])
        for n, (src, dst) in enumerate(
            (
                (routes_h, routes), (x_h, x), (cg_h, cg), (ci_h, ci), (bg_h, bg), (taps_h, taps), (mixw, mw_v),
                (rw_h, rw), (gain_h, gain), (wg.at[0], wg_v), (wu.at[0], wu_v), (wd.at[0], wd_v),
            )
        )
    ]
    for load in loads:
        load.start()

    loads[0].wait()
    e = routes[...]
    dz = (e // S + NZ - iz) & (NZ - 1)
    chunk = jnp.zeros_like(e)
    for n in range(NZ):
        chunk = jnp.where(dz == order[n], n, chunk)
    dx = ((e >> 1) + NX - ix) & (NX - 1)
    dc = (e + ic) & 1
    k = chunk * S + dx * 2 + dc
    hot = [iota((n_ep, ntok), 0) == k[q : q + 1] for q in range(2)]
    named = jnp.where(hot[0] | hot[1], 1.0, 0.0).astype(BF)
    before = jnp.where(iota((ntok, ntok), 0) < iota((ntok, ntok), 1), 1.0, 0.0).astype(BF)
    rank = jnp.dot(named, before, preferred_element_type=F32)
    marks = []
    for q in range(2):
        slot = jnp.sum(jnp.where(hot[q], rank, 0.0), axis=0, keepdims=True).astype(jnp.int32)
        kq = k[q : q + 1]
        marks.append(
            (jnp.where(slot < 8, kq * 8 + slot, -1), jnp.where(slot >= 8, kq * 4 + slot - 8, -1))
        )
    ia = iota((n_ep * 8, ntok), 0)
    ib = iota((n_ep * 4, ntok), 0)
    pa = jnp.where((ia == marks[0][0]) | (ia == marks[1][0]), 1.0, 0.0).astype(BF)
    pb = jnp.where((ib == marks[0][1]) | (ib == marks[1][1]), 1.0, 0.0).astype(BF)
    loads[1].wait()
    xv = x[...]
    oa = jnp.dot(pa, xv, preferred_element_type=F32).reshape(n_ep, 8, DS).astype(BF)
    out[:, :, :DS] = oa
    even, odd = to_message(jnp.dot(pb, xv, preferred_element_type=F32), n_ep)
    for p in range(n_ep // 2):
        out[2 * p, :, DS:] = even[p].astype(BF)
        out[2 * p + 1, :, DS:] = odd[p].astype(BF)
    G[0, 0, 0] = out[0]

    for load in loads[2:7]:
        load.wait()
    mrows = MS.shape[1]
    mh = mrows // 2
    prod = cg[...].astype(F32) * ci[...].astype(F32)
    back1 = pltpu.roll(prod, 1, axis=0)
    back2 = pltpu.roll(prod, 2, axis=0)
    tv = taps[...]
    conv = tv[0:1] * back2 + tv[1:2] * back1 + tv[2:3] * prod
    gated = (bg[...].astype(F32) * conv).astype(BF)
    for q in range(1, TP):
        MS[q] = jnp.dot(
            gated[q * mrows : (q + 1) * mrows], mw_v[...], preferred_element_type=F32
        ).astype(BF)

    pl.semaphore_wait(barrier, n_ep - 1 + 2)

    ntail = cg.shape[0] - 8
    tails = [
        remote(ref.at[pl.ds(ntail, 8)], halo.at[q], halo_s.at[q], halo_r.at[q], ep=(i + 1) & (n_ep - 1))
        for q, ref in enumerate((cg, ci))
    ]
    for tail in tails:
        tail.start()

    for c in range(NZ):
        for r in range(S):
            if c + r:
                remote(
                    out.at[c * S + r], G.at[0, c, r], disp_s, disp_r.at[c], ep=device(order[c], r // 2, r % 2)
                ).start()

    for tail in tails:
        tail.wait_recv()
    prev = halo[0].astype(F32) * halo[1].astype(F32)
    prev = jnp.where(i > 0, prev, 0.0)
    row = iota((mrows, prod.shape[1]), 0)
    first1 = jnp.where(row == 0, prev[7:8], back1[:mrows])
    first2 = jnp.where(row == 0, prev[6:7], jnp.where(row == 1, prev[7:8], back2[:mrows]))
    conv = tv[0:1] * first2 + tv[1:2] * first1 + tv[2:3] * prod[:mrows]
    gated = (bg[pl.ds(0, mrows), :].astype(F32) * conv).astype(BF)
    MS[0] = jnp.dot(gated, mw_v[...], preferred_element_type=F32).astype(BF)
    for d, other in sides:
        remote(
            MS.at[far, pl.ds(d * mh, mh)], MR1.at[d], m1_s.at[d], m1_r.at[d], tp=other
        ).start()
        keep = (1 - d) * mh
        remote(
            MS.at[other, pl.ds(keep, mh)], MF.at[d, pl.ds(keep, mh)], mi_s.at[d], mi_r.at[d], tp=other
        ).start()

    loads[7].wait()
    loads[8].wait()
    table = jnp.concatenate(
        [marks[0][0].astype(F32), marks[1][0].astype(F32), marks[0][1].astype(F32), marks[1][1].astype(F32), rw[...]]
        + [jnp.zeros((122, ntok), F32)],
        axis=0,
    )
    cols = jnp.transpose(table)
    ga = iota((ntok, n_ep * 8), 1)
    gb = iota((ntok, n_ep * 4), 1)
    for q in range(2):
        pick_a[q] = jnp.where(ga == cols[:, q : q + 1].astype(jnp.int32), 1.0, 0.0).astype(BF)
        pick_b[q] = jnp.where(gb == cols[:, 2 + q : 3 + q].astype(jnp.int32), 1.0, 0.0).astype(BF)
    share = [cols[:, 4 + q : 5 + q] for q in range(2)]

    def stage_direct(c):
        @pl.when(c == 0)
        def _():
            arrived(G.at[0, 0, pl.ds(1, S - 1)], disp_r.at[0])

        @pl.when(c > 0)
        def _():
            arrived(G.at[0, c], disp_r.at[c])

        for d, other in sides:
            remote(G.at[0, c], G.at[1 + d, c], gd_s.at[d], gd_r.at[d, c], tp=other).start()

    def stage_relay(c):
        for d, other in sides:
            arrived(G.at[1 + d, c], gd_r.at[d, c])
            half = pl.ds(d * H, H)
            remote(G.at[1 + d, c, half], G.at[3, c, half], gr_s.at[d], gr_r.at[d, c], tp=other).start()

    def stage_expert(c):
        @pl.when(c == 0)
        def _():
            for load in loads[9:]:
                load.wait()

        for d in range(2):
            arrived(G.at[3, c, pl.ds(d * H, H)], gr_r.at[d, c])
        owners = (y, down, up, far)
        total = jnp.zeros((S, 8, 1), F32)
        total_b = jnp.zeros((S, 8, 1), F32)
        for n in range(TP):
            g = G[n, c].astype(F32)
            a, b = g[:, :, :DS], g[:, :, DS:]
            total = total + jnp.sum(a * a, axis=2, keepdims=True)
            total_b = total_b + jnp.sum(b * b, axis=2, keepdims=True)
        width = DS * TP
        total_b = total_b + pltpu.roll(total_b, 4, axis=1)
        sa = lax.rsqrt(total / width + 1e-06)
        sb = lax.rsqrt(total_b / width + 1e-06)
        for n, owner in enumerate(owners):
            g = G[n, c].astype(F32)
            gn = gain[owner]
            nrm[owner, pl.ds(0, ar), :] = (g[:, :, :DS] * sa).reshape(ar, DS).astype(F32) * gn
            v0, v1 = from_message(g[:, :, DS:] * sb, S)
            nrm[owner, pl.ds(ar, rows - ar), pl.ds(0, h)] = v0 * gn[:, :h]
            nrm[owner, pl.ds(ar, rows - ar), pl.ds(h, h)] = v1 * gn[:, h:]
        lhs = jnp.concatenate([nrm[n].astype(BF) for n in range(TP)], axis=1)
        gate = jnp.dot(lhs, wg_v[...], preferred_element_type=F32)
        upper = jnp.dot(lhs, wu_v[...], preferred_element_type=F32)
        hidden = (gate / (1.0 + jnp.exp(-gate)) * upper).astype(BF)
        for q in range(TP):
            part = jnp.dot(hidden, wd_v[:, q * DS : (q + 1) * DS], preferred_element_type=F32)
            PS[c, q, :, :, pl.ds(0, DS)] = part[:ar].reshape(S, 8, DS).astype(BF)
            even, odd = to_message(part[ar:], S)
            for p in range(H):
                PS[c, q, 2 * p, :, pl.ds(DS, h)] = even[p].astype(BF)
                PS[c, q, 2 * p + 1, :, pl.ds(DS, h)] = odd[p].astype(BF)
        for d, other in sides:
            half, rest = pl.ds(d * H, H), pl.ds((1 - d) * H, H)
            remote(PS.at[c, far, half], R1.at[d, c], r1_s.at[d], r1_r.at[d, c], tp=other).start()
            remote(PS.at[c, other, rest], FR.at[d, c, rest], fi_s.at[d], fi_r.at[d, c], tp=other).start()

    def stage_add(c):
        for d, other in sides:
            half = pl.ds(d * H, H)
            arrived(R1.at[d, c], r1_r.at[d, c])
            ACC[d, c] = (PS[c, other, half].astype(F32) + R1[d, c].astype(F32)).astype(BF)
            remote(ACC.at[d, c], FR.at[d, c, half], fa_s.at[d], fa_r.at[d, c], tp=other).start()

    def stage_back(c):
        for d in range(2):
            arrived(FR.at[d, c, pl.ds((1 - d) * H, H)], fi_r.at[d, c])
            arrived(FR.at[d, c, pl.ds(d * H, H)], fa_r.at[d, c])
        whole = PS[c, y].astype(F32) + FR[0, c].astype(F32) + FR[1, c].astype(F32)
        FIN[c] = whole.astype(BF)

        @pl.when(c == 0)
        def _():
            ret[0, 0] = FIN[0, 0]

        dz = NZ - dz_of(c)
        for r in range(S):
            send = remote(
                FIN.at[c, r], ret.at[c, r], back_s, back_r.at[c], ep=device(dz, NX - r // 2, r % 2)
            )
            if r:
                send.start()
            else:
                pl.when(c > 0)(send.start)

    @pl.loop(-3, NZ + 2)
    def _(u):
        @pl.when((u >= -1) & (u < NZ - 1))
        def _():
            stage_relay(u + 1)

        @pl.when(u < NZ - 3)
        def _():
            stage_direct(u + 3)

        @pl.when((u >= 1) & (u < NZ + 1))
        def _():
            stage_add(u - 1)

        @pl.when(u >= 2)
        def _():
            stage_back(u - 2)

        @pl.when((u >= 0) & (u < NZ))
        def _():
            stage_expert(u)

        @pl.when(u == NZ - 2)
        def _():
            for d, other in sides:
                half = pl.ds(d * mh, mh)
                arrived(MR1.at[d], m1_r.at[d])
                MACC[d] = (MS[other, half].astype(F32) + MR1[d].astype(F32)).astype(BF)
                remote(MACC.at[d], MF.at[d, half], ma_s.at[d], ma_r.at[d], tp=other).start()

    for d in range(2):
        arrived(MF.at[d, pl.ds((1 - d) * mh, mh)], mi_r.at[d])
        arrived(MF.at[d, pl.ds(d * mh, mh)], ma_r.at[d])
    mixed[...] = (MS[y].astype(F32) + MF[0].astype(F32) + MF[1].astype(F32)).astype(BF)

    arrived(ret.at[0, pl.ds(1, S - 1)], back_r.at[0])
    for c in range(1, NZ):
        arrived(ret.at[c], back_r.at[c])
    back = ret[...].reshape(n_ep, 8, DS + h)
    ra = back[:, :, :DS].reshape(n_ep * 8, DS)
    b0, b1 = from_message(back[:, :, DS:].astype(F32), n_ep)
    rb = jnp.concatenate([b0, b1], axis=1).astype(BF)
    total = jnp.zeros((ntok, DS), F32)
    for q in range(2):
        row = jnp.dot(pick_a[q], ra, preferred_element_type=F32)
        row = row + jnp.dot(pick_b[q], rb, preferred_element_type=F32)
        total = total + row * share[q]
    routed[...] = total.astype(BF)

    for tail in tails:
        tail.wait_send()
    left(out.at[pl.ds(1, n_ep - 1)], disp_s)
    left(out.at[pl.ds(1, n_ep - 1)], back_s)
    for d in range(2):
        left(G.at[0], gd_s.at[d])
        left(R1.at[0], gr_s.at[d])
        left(R1.at[0], r1_s.at[d])
        left(R1.at[0], fi_s.at[d])
        left(R1.at[0], fa_s.at[d])
        left(MR1.at[0], m1_s.at[d])
        left(MR1.at[0], mi_s.at[d])
        left(MR1.at[0], ma_s.at[d])


def body(mix_bgate, mix_cgate, mix_input, conv_taps, mix_out_w, moe_x, moe_gain, routes, route_w, w_gate, w_up, w_down, *, dims):
    NZ, NX, order = dims
    S = NX * 2
    H = S // 2
    n_ep = NZ * S
    ntok, DS = moe_x.shape
    D = DS * TP
    F = w_gate.shape[2]
    CH = mix_out_w.shape[0]
    ML = DS + DS // 2
    length = mix_input.shape[0]
    mrows = length // TP
    vmem = pl.BlockSpec(memory_space=pltpu.VMEM)
    hbm = pl.BlockSpec(memory_space=pltpu.HBM)
    V = pltpu.VMEM
    dma = pltpu.SemaphoreType.DMA
    return pl.pallas_call(
        functools.partial(kernel, dims),
        name="step",
        out_shape=(
            V((mrows, D), BF),
            V((ntok, DS), BF),
        ),
        in_specs=[hbm] * 12,
        out_specs=(vmem, vmem),
        scratch_shapes=[
            V((length, CH), BF), V((length, CH), BF), V((length, CH), BF), V((3, CH), F32),
            V((ntok, DS), BF), V((TP, 1, DS), F32), V((2, ntok), jnp.int32), V((2, ntok), F32),
            V((D, F), BF), V((D, F), BF), V((F, D), BF), V((CH, D), BF),
            V((n_ep, 8, ML), BF),
            V((4, NZ, S, 8, ML), BF),
            V((TP, S * CAP, DS), F32),
            V((NZ, TP, S, 8, ML), BF),
            V((2, NZ, H, 8, ML), BF),
            V((2, NZ, S, 8, ML), BF),
            V((2, NZ, H, 8, ML), BF),
            V((NZ, S, 8, ML), BF),
            V((NZ, S, 8, ML), BF),
            V((2, 8, CH), BF),
            V((TP, mrows, D), BF),
            V((2, mrows // 2, D), BF),
            V((2, mrows, D), BF),
            V((2, mrows // 2, D), BF),
            V((2, ntok, n_ep * 8), BF), V((2, ntok, n_ep * 4), BF),
            dma((12,)), dma((2,)), dma((2,)),
            dma, dma((NZ,)),
            dma((2,)), dma((2, NZ)), dma((2,)), dma((2, NZ)),
            dma((2,)), dma((2, NZ)), dma((2,)), dma((2, NZ)), dma((2,)), dma((2, NZ)),
            dma, dma((NZ,)),
            dma((2,)), dma((2,)), dma((2,)), dma((2,)), dma((2,)), dma((2,)),
        ],
        compiler_params=pltpu.CompilerParams(
            collective_id=0, has_side_effects=True, vmem_limit_bytes=67043328 - 2 * 2 * mrows * D - 16384
        ),
    )(
        mix_bgate, mix_cgate, mix_input, conv_taps, mix_out_w, moe_x,
        moe_gain.reshape(TP, 1, DS), routes.T, route_w.T, w_gate, w_up, w_down,
    )


def solution(mesh):
    n_ep = mesh.shape["ep"]
    NZ, NX = (8, n_ep // 16) if n_ep >= 32 else (2, n_ep // 4)
    order = (0, 1, 6, 3, 5, 4, 2, 7) if NZ == 8 else tuple(range(NZ))
    in_specs = (
        P("ep", "tp"), P("ep", "tp"), P("ep", "tp"), P(None, "tp"), P("tp", None), P("ep", "tp"), P(),
        P("ep", None), P("ep", None), P("ep", None, "tp"), P("ep", None, "tp"), P("ep", "tp", None),
    )
    out_specs = (P(("ep", "tp"), None), P("ep", "tp"))
    return jax.shard_map(
        functools.partial(body, dims=(NZ, NX, order)),
        mesh=mesh, in_specs=in_specs, out_specs=out_specs, check_vma=False,
    )
```

```python
import functools

import jax
import jax.numpy as jnp
from jax import lax
from jax.experimental import pallas as pl
from jax.experimental.pallas import tpu as pltpu
from jax.sharding import PartitionSpec as P

CAP = 12
TP = 4
BF = jnp.bfloat16
F32 = jnp.float32


def iota(shape, dim):
    return lax.broadcasted_iota(jnp.int32, shape, dim)


def to_message(v, groups):
    h = v.shape[1] // 2
    v0 = v[:, :h].reshape(groups // 2, 8, h)
    v1 = v[:, h:].reshape(groups // 2, 8, h)
    low = iota(v0.shape, 1) < 4
    even = jnp.where(low, v0, pltpu.roll(v1, 4, axis=1))
    odd = jnp.where(low, pltpu.roll(v0, 4, axis=1), v1)
    return even, odd


def from_message(m, groups):
    h = m.shape[2]
    pairs = m.reshape(groups // 2, 2, 8, h)
    even, odd = pairs[:, 0], pairs[:, 1]
    low = iota(even.shape, 1) < 4
    v0 = jnp.where(low, even, pltpu.roll(odd, 4, axis=1))
    v1 = jnp.where(low, pltpu.roll(even, 4, axis=1), odd)
    return v0.reshape(groups * 4, h), v1.reshape(groups * 4, h)


def kernel(
    dims,
    bg_h, cg_h, ci_h, taps_h, mixw, x_h, gain_h, routes_h, rw_h, wg, wu, wd,
    mixed, routed,
    bg, cg, ci, taps, x, gain, routes, rw,
    wg_v, wu_v, wd_v, mw_v, out, G, nrm, PS, R1, FR, ACC, FIN, ret,
    halo, MS, MR1, MF, MACC, XS, XR1, XF, XACC, XO, pick_a, pick_b,
    wsem, halo_s, halo_r, disp_s, disp_r, gd_s, gd_r, gr_s, gr_r,
    r1_s, r1_r, fi_s, fi_r, fa_s, fa_r, back_s, back_r,
    m1_s, m1_r, mi_s, mi_r, ma_s, ma_r, x1_s, x1_r, xi_s, xi_r, xa_s, xa_r, xin_s, xin_r, xo_s, xo_r,
):
    NZ, NX, orders = dims
    S = NX * 2
    H = S // 2
    n_ep = NZ * S
    ntok, DS = x.shape
    h = DS // 2
    rows = S * CAP
    ar = S * 8
    i = lax.axis_index("ep")
    y = lax.axis_index("tp")
    up = (y + 1) & (TP - 1)
    down = (y + 3) & (TP - 1)
    far = (y + 2) & (TP - 1)
    ic = i & 1
    ix = (i >> 1) & (NX - 1)
    iz = i // S
    sides = ((0, up), (1, down))

    def device(dz, dx, dc):
        return ((((iz + dz) & (NZ - 1)) * NX + ((ix + dx) & (NX - 1))) << 1) + ((ic + dc) & 1)

    taken, place = jnp.int32(0), jnp.int32(0)
    for n in range(NZ):
        taken = jnp.where(iz == n, sum(p << 4 * c for c, p in enumerate(orders[n])), taken)
        place = jnp.where(iz == n, sum(orders[e].index(n) << 4 * e for e in range(NZ)), place)

    def remote(src, dst, ssem, rsem, ep=None, tp=None):
        return pltpu.make_async_remote_copy(
            src_ref=src, dst_ref=dst, send_sem=ssem, recv_sem=rsem,
            device_id=(i if ep is None else ep, y if tp is None else tp),
            device_id_type=pl.DeviceIdType.MESH,
        )

    def arrived(ref, sem):
        remote(ref, ref, sem, sem, tp=up).wait_recv()

    def left(ref, sem):
        remote(ref, ref, sem, sem, tp=up).wait_send()

    barrier = pltpu.get_barrier_semaphore()

    def greet(ep, tp):
        pl.semaphore_signal(barrier, inc=1, device_id=(ep, tp), device_id_type=pl.DeviceIdType.MESH)

    for dz in sorted(range(NZ), key=lambda n: -min(n, NZ - n)):
        for r in range(S):
            if dz + r:
                greet(device(dz, r // 2, r % 2), y)
    for _, other in sides:
        greet(i, other)

    loads = [
        pltpu.make_async_copy(src, dst, wsem.at[n])
        for n, (src, dst) in enumerate(
            (
                (routes_h, routes), (x_h, x), (cg_h, cg), (ci_h, ci), (bg_h, bg), (taps_h, taps), (mixw, mw_v),
                (rw_h, rw), (gain_h, gain), (wg.at[0], wg_v), (wu.at[0], wu_v), (wd.at[0], wd_v),
            )
        )
    ]
    for load in loads:
        load.start()

    loads[0].wait()
    e = routes[...]
    dz = (e // S + NZ - iz) & (NZ - 1)
    dx = ((e >> 1) + NX - ix) & (NX - 1)
    dc = (e + ic) & 1
    k = dz * S + dx * 2 + dc
    hot = [iota((n_ep, ntok), 0) == k[q : q + 1] for q in range(2)]
    named = jnp.where(hot[0] | hot[1], 1.0, 0.0).astype(BF)
    before = jnp.where(iota((ntok, ntok), 0) < iota((ntok, ntok), 1), 1.0, 0.0).astype(BF)
    rank = jnp.dot(named, before, preferred_element_type=F32)
    marks = []
    for q in range(2):
        slot = jnp.sum(jnp.where(hot[q], rank, 0.0), axis=0, keepdims=True).astype(jnp.int32)
        kq = k[q : q + 1]
        marks.append(
            (jnp.where(slot < 8, kq * 8 + slot, -1), jnp.where(slot >= 8, kq * 4 + slot - 8, -1))
        )
    ia = iota((n_ep * 8, ntok), 0)
    ib = iota((n_ep * 4, ntok), 0)
    pa = jnp.where((ia == marks[0][0]) | (ia == marks[1][0]), 1.0, 0.0).astype(BF)
    pb = jnp.where((ib == marks[0][1]) | (ib == marks[1][1]), 1.0, 0.0).astype(BF)
    loads[1].wait()
    xv = x[...]
    oa = jnp.dot(pa, xv, preferred_element_type=F32).reshape(n_ep, 8, DS).astype(BF)
    out[:, :, :DS] = oa
    even, odd = to_message(jnp.dot(pb, xv, preferred_element_type=F32), n_ep)
    for p in range(n_ep // 2):
        out[2 * p, :, DS:] = even[p].astype(BF)
        out[2 * p + 1, :, DS:] = odd[p].astype(BF)
    G[0, 0, 0] = out[0]

    for load in loads[2:7]:
        load.wait()
    groups, more = MS.shape[1], XS.shape[1] // 2
    mrows = (groups + more) * 8
    buddy = i + 1 - 2 * ic
    prod = cg[...].astype(F32) * ci[...].astype(F32)
    back1 = pltpu.roll(prod, 1, axis=0)
    back2 = pltpu.roll(prod, 2, axis=0)
    tv = taps[...]
    conv = tv[0:1] * back2 + tv[1:2] * back1 + tv[2:3] * prod
    gated = (bg[...].astype(F32) * conv).astype(BF)
    for q in range(TP):
        product = jnp.dot(gated[q * mrows : (q + 1) * mrows], mw_v[...], preferred_element_type=F32)
        product = product.reshape(groups + more, 8, product.shape[1]).astype(BF)
        if q:
            MS[q] = product[:groups]
        XS[q, pl.ds(0, more)] = product[groups:]

    pl.semaphore_wait(barrier, n_ep - 1 + 2)

    ntail = cg.shape[0] - 8
    tails = [
        remote(ref.at[pl.ds(ntail, 8)], halo.at[q], halo_s.at[q], halo_r.at[q], ep=(i + 1) & (n_ep - 1))
        for q, ref in enumerate((cg, ci))
    ]
    def begin(own, first, last, size, sems, ready):
        half = size // 2
        for d, other in sides:
            keep = (1 - d) * half

            @pl.when(ready(far))
            def _():
                remote(
                    own.at[far, pl.ds(d * half, half)], first.at[d], sems[0].at[d], sems[1].at[d], tp=other
                ).start()

            @pl.when(ready(other))
            def _():
                remote(
                    own.at[other, pl.ds(keep, half)], last.at[d, pl.ds(keep, half)], sems[2].at[d], sems[3].at[d],
                    tp=other,
                ).start()

    m_sems = (m1_s, m1_r, mi_s, mi_r, ma_s, ma_r)
    x_sems = (x1_s, x1_r, xi_s, xi_r, xa_s, xa_r)
    for tail in tails:
        tail.start()
    begin(MS, MR1, MF, groups, m_sems, lambda q: q > 0)

    handed = [
        remote(XS.at[q, pl.ds(0, more)], XS.at[q, pl.ds(more, more)], xin_s.at[q], xin_r.at[q], ep=buddy)
        for q in range(TP)
    ]

    @pl.when(ic == 0)
    def _():
        for hand in handed:
            hand.start()

    for dz in sorted(range(NZ), key=lambda n: min(n, NZ - n)):
        c = (place >> (((iz + dz) & (NZ - 1)) * 4)) & 15 if dz else 0
        for r in range(S):
            if dz + r:
                remote(
                    out.at[dz * S + r], G.at[0, c, r], disp_s, disp_r.at[c], ep=device(dz, r // 2, r % 2)
                ).start()

    for tail in tails:
        tail.wait_recv()
    prev = halo[0].astype(F32) * halo[1].astype(F32)
    prev = jnp.where(i > 0, prev, 0.0)
    row = iota((mrows, prod.shape[1]), 0)
    first1 = jnp.where(row == 0, prev[7:8], back1[:mrows])
    first2 = jnp.where(row == 0, prev[6:7], jnp.where(row == 1, prev[7:8], back2[:mrows]))
    conv = tv[0:1] * first2 + tv[1:2] * first1 + tv[2:3] * prod[:mrows]
    gated = (bg[pl.ds(0, mrows), :].astype(F32) * conv).astype(BF)
    product = jnp.dot(gated, mw_v[...], preferred_element_type=F32)
    MS[0] = product.reshape(groups + more, 8, product.shape[1])[:groups].astype(BF)

    def pass_on(own, first, last, added, size, sems):
        half = size // 2
        for d, other in sides:
            part = pl.ds(d * half, half)
            arrived(first.at[d], sems[1].at[d])
            added[d] = (own[other, part].astype(F32) + first[d].astype(F32)).astype(BF)
            remote(added.at[d], last.at[d, part], sems[4].at[d], sems[5].at[d], tp=other).start()

    def summed(own, last, size, sems):
        half = size // 2
        for d in range(2):
            arrived(last.at[d, pl.ds((1 - d) * half, half)], sems[3].at[d])
            arrived(last.at[d, pl.ds(d * half, half)], sems[5].at[d])
        return (own[y].astype(F32) + last[0].astype(F32) + last[1].astype(F32)).astype(BF)

    begin(MS, MR1, MF, groups, m_sems, lambda q: q == 0)

    @pl.when(ic == 1)
    def _():
        for hand in handed:
            hand.wait_recv()
        begin(XS, XR1, XF, 2 * more, x_sems, lambda q: q >= 0)

    loads[7].wait()
    loads[8].wait()
    table = jnp.concatenate(
        [marks[0][0].astype(F32), marks[1][0].astype(F32), marks[0][1].astype(F32), marks[1][1].astype(F32), rw[...]]
        + [jnp.zeros((122, ntok), F32)],
        axis=0,
    )
    cols = jnp.transpose(table)
    ga = iota((ntok, n_ep * 8), 1)
    gb = iota((ntok, n_ep * 4), 1)
    for q in range(2):
        pick_a[q] = jnp.where(ga == cols[:, q : q + 1].astype(jnp.int32), 1.0, 0.0).astype(BF)
        pick_b[q] = jnp.where(gb == cols[:, 2 + q : 3 + q].astype(jnp.int32), 1.0, 0.0).astype(BF)
    share = [cols[:, 4 + q : 5 + q] for q in range(2)]

    def stage_direct(c):
        @pl.when(c == 0)
        def _():
            arrived(G.at[0, 0, pl.ds(1, S - 1)], disp_r.at[0])

        @pl.when(c > 0)
        def _():
            arrived(G.at[0, c], disp_r.at[c])

        for d, other in sides:
            remote(G.at[0, c], G.at[1 + d, c], gd_s.at[d], gd_r.at[d, c], tp=other).start()

    def stage_relay(c):
        for d, other in sides:
            arrived(G.at[1 + d, c], gd_r.at[d, c])
            half = pl.ds(d * H, H)
            remote(G.at[1 + d, c, half], G.at[3, c, half], gr_s.at[d], gr_r.at[d, c], tp=other).start()

    def stage_expert(c):
        @pl.when(c == 0)
        def _():
            for load in loads[9:]:
                load.wait()

        for d in range(2):
            arrived(G.at[3, c, pl.ds(d * H, H)], gr_r.at[d, c])
        owners = (y, down, up, far)
        total = jnp.zeros((S, 8, 1), F32)
        total_b = jnp.zeros((S, 8, 1), F32)
        for n in range(TP):
            g = G[n, c].astype(F32)
            a, b = g[:, :, :DS], g[:, :, DS:]
            total = total + jnp.sum(a * a, axis=2, keepdims=True)
            total_b = total_b + jnp.sum(b * b, axis=2, keepdims=True)
        width = DS * TP
        total_b = total_b + pltpu.roll(total_b, 4, axis=1)
        sa = lax.rsqrt(total / width + 1e-06)
        sb = lax.rsqrt(total_b / width + 1e-06)
        for n, owner in enumerate(owners):
            g = G[n, c].astype(F32)
            gn = gain[owner]
            nrm[owner, pl.ds(0, ar), :] = (g[:, :, :DS] * sa).reshape(ar, DS).astype(F32) * gn
            v0, v1 = from_message(g[:, :, DS:] * sb, S)
            nrm[owner, pl.ds(ar, rows - ar), pl.ds(0, h)] = v0 * gn[:, :h]
            nrm[owner, pl.ds(ar, rows - ar), pl.ds(h, h)] = v1 * gn[:, h:]
        lhs = jnp.concatenate([nrm[n].astype(BF) for n in range(TP)], axis=1)
        gate = jnp.dot(lhs, wg_v[...], preferred_element_type=F32)
        upper = jnp.dot(lhs, wu_v[...], preferred_element_type=F32)
        hidden = (gate / (1.0 + jnp.exp(-gate)) * upper).astype(BF)
        for q in range(TP):
            part = jnp.dot(hidden, wd_v[:, q * DS : (q + 1) * DS], preferred_element_type=F32)
            PS[c, q, :, :, pl.ds(0, DS)] = part[:ar].reshape(S, 8, DS).astype(BF)
            even, odd = to_message(part[ar:], S)
            for p in range(H):
                PS[c, q, 2 * p, :, pl.ds(DS, h)] = even[p].astype(BF)
                PS[c, q, 2 * p + 1, :, pl.ds(DS, h)] = odd[p].astype(BF)
        for d, other in sides:
            half, rest = pl.ds(d * H, H), pl.ds((1 - d) * H, H)
            remote(PS.at[c, far, half], R1.at[d, c], r1_s.at[d], r1_r.at[d, c], tp=other).start()
            remote(PS.at[c, other, rest], FR.at[d, c, rest], fi_s.at[d], fi_r.at[d, c], tp=other).start()

    def stage_add(c):
        for d, other in sides:
            half = pl.ds(d * H, H)
            arrived(R1.at[d, c], r1_r.at[d, c])
            ACC[d, c] = (PS[c, other, half].astype(F32) + R1[d, c].astype(F32)).astype(BF)
            remote(ACC.at[d, c], FR.at[d, c, half], fa_s.at[d], fa_r.at[d, c], tp=other).start()

    def stage_back(c):
        for d in range(2):
            arrived(FR.at[d, c, pl.ds((1 - d) * H, H)], fi_r.at[d, c])
            arrived(FR.at[d, c, pl.ds(d * H, H)], fa_r.at[d, c])
        whole = PS[c, y].astype(F32) + FR[0, c].astype(F32) + FR[1, c].astype(F32)
        FIN[c] = whole.astype(BF)

        @pl.when(c == 0)
        def _():
            ret[0, 0] = FIN[0, 0]

        plane = (taken >> (4 * c)) & 15
        dz = (iz - plane) & (NZ - 1)
        for r in range(S):
            send = remote(
                FIN.at[c, r], ret.at[dz, r], back_s, back_r.at[dz], ep=device(NZ - dz, NX - r // 2, r % 2)
            )
            if r:
                send.start()
            else:
                pl.when(c > 0)(send.start)

    @pl.loop(-3, NZ + 2)
    def _(u):
        @pl.when((u >= -1) & (u < NZ - 1))
        def _():
            stage_relay(u + 1)

        @pl.when(u < NZ - 3)
        def _():
            stage_direct(u + 3)

        @pl.when((u >= 0) & (u < NZ))
        def _():
            stage_expert(u)

        @pl.when((u >= 1) & (u < NZ + 1))
        def _():
            stage_add(u - 1)

        @pl.when(u >= 2)
        def _():
            stage_back(u - 2)

        @pl.when(u == NZ - 2)
        def _():
            pass_on(MS, MR1, MF, MACC, groups, m_sems)

            @pl.when(ic == 1)
            def _():
                pass_on(XS, XR1, XF, XACC, 2 * more, x_sems)

    kept = groups * 8
    mixed[pl.ds(0, kept), :] = summed(MS, MF, groups, m_sems).reshape(kept, -1)
    result = remote(XO.at[0], XO.at[1], xo_s, xo_r, ep=buddy)

    @pl.when(ic == 1)
    def _():
        both = summed(XS, XF, 2 * more, x_sems)
        XO[0] = both[more:]
        result.start()
        mixed[pl.ds(kept, mrows - kept), :] = both[:more].reshape(mrows - kept, -1)

    @pl.when(ic == 0)
    def _():
        result.wait_recv()
        mixed[pl.ds(kept, mrows - kept), :] = XO[1].reshape(mrows - kept, -1)

    arrived(ret.at[0, pl.ds(1, S - 1)], back_r.at[0])
    for c in range(1, NZ):
        arrived(ret.at[c], back_r.at[c])
    back = ret[...].reshape(n_ep, 8, DS + h)
    ra = back[:, :, :DS].reshape(n_ep * 8, DS)
    b0, b1 = from_message(back[:, :, DS:].astype(F32), n_ep)
    rb = jnp.concatenate([b0, b1], axis=1).astype(BF)
    total = jnp.zeros((ntok, DS), F32)
    for q in range(2):
        row = jnp.dot(pick_a[q], ra, preferred_element_type=F32)
        row = row + jnp.dot(pick_b[q], rb, preferred_element_type=F32)
        total = total + row * share[q]
    routed[...] = total.astype(BF)

    for tail in tails:
        tail.wait_send()
    left(out.at[pl.ds(1, n_ep - 1)], disp_s)
    left(out.at[pl.ds(1, n_ep - 1)], back_s)
    for d in range(2):
        left(G.at[0], gd_s.at[d])
        left(R1.at[0], gr_s.at[d])
        left(R1.at[0], r1_s.at[d])
        left(R1.at[0], fi_s.at[d])
        left(R1.at[0], fa_s.at[d])
        left(MR1.at[0], m1_s.at[d])
        left(MR1.at[0], mi_s.at[d])
        left(MR1.at[0], ma_s.at[d])

    @pl.when(ic == 1)
    def _():
        result.wait_send()
        for d in range(2):
            left(XR1.at[0], x1_s.at[d])
            left(XR1.at[0], xi_s.at[d])
            left(XR1.at[0], xa_s.at[d])

    @pl.when(ic == 0)
    def _():
        for hand in handed:
            hand.wait_send()


def body(mix_bgate, mix_cgate, mix_input, conv_taps, mix_out_w, moe_x, moe_gain, routes, route_w, w_gate, w_up, w_down, *, dims):
    NZ, NX, _ = dims
    S = NX * 2
    H = S // 2
    n_ep = NZ * S
    ntok, DS = moe_x.shape
    D = DS * TP
    F = w_gate.shape[2]
    CH = mix_out_w.shape[0]
    ML = DS + DS // 2
    length = mix_input.shape[0]
    mrows = length // TP
    more = mrows // 16
    groups = mrows // 8 - more
    vmem = pl.BlockSpec(memory_space=pltpu.VMEM)
    hbm = pl.BlockSpec(memory_space=pltpu.HBM)
    V = pltpu.VMEM
    dma = pltpu.SemaphoreType.DMA
    return pl.pallas_call(
        functools.partial(kernel, dims),
        name="step",
        out_shape=(
            V((mrows, D), BF),
            V((ntok, DS), BF),
        ),
        in_specs=[hbm] * 12,
        out_specs=(vmem, vmem),
        scratch_shapes=[
            V((length, CH), BF), V((length, CH), BF), V((length, CH), BF), V((3, CH), F32),
            V((ntok, DS), BF), V((TP, 1, DS), F32), V((2, ntok), jnp.int32), V((2, ntok), F32),
            V((D, F), BF), V((D, F), BF), V((F, D), BF), V((CH, D), BF),
            V((n_ep, 8, ML), BF),
            V((4, NZ, S, 8, ML), BF),
            V((TP, S * CAP, DS), F32),
            V((NZ, TP, S, 8, ML), BF),
            V((2, NZ, H, 8, ML), BF),
            V((2, NZ, S, 8, ML), BF),
            V((2, NZ, H, 8, ML), BF),
            V((NZ, S, 8, ML), BF),
            V((NZ, S, 8, ML), BF),
            V((2, 8, CH), BF),
            V((TP, groups, 8, D), BF),
            V((2, groups // 2, 8, D), BF),
            V((2, groups, 8, D), BF),
            V((2, groups // 2, 8, D), BF),
            V((TP, 2 * more, 8, D), BF),
            V((2, more, 8, D), BF),
            V((2, 2 * more, 8, D), BF),
            V((2, more, 8, D), BF),
            V((2, more, 8, D), BF),
            V((2, ntok, n_ep * 8), BF), V((2, ntok, n_ep * 4), BF),
            dma((12,)), dma((2,)), dma((2,)),
            dma, dma((NZ,)),
            dma((2,)), dma((2, NZ)), dma((2,)), dma((2, NZ)),
            dma((2,)), dma((2, NZ)), dma((2,)), dma((2, NZ)), dma((2,)), dma((2, NZ)),
            dma, dma((NZ,)),
            dma((2,)), dma((2,)), dma((2,)), dma((2,)), dma((2,)), dma((2,)),
            dma((2,)), dma((2,)), dma((2,)), dma((2,)), dma((2,)), dma((2,)),
            dma((TP,)), dma((TP,)), dma, dma,
        ],
        compiler_params=pltpu.CompilerParams(
            collective_id=0, has_side_effects=True, vmem_limit_bytes=67043328 - 2 * 2 * mrows * D - 16384
        ),
    )(
        mix_bgate, mix_cgate, mix_input, conv_taps, mix_out_w, moe_x,
        moe_gain.reshape(TP, 1, DS), routes.T, route_w.T, w_gate, w_up, w_down,
    )


def solution(mesh):
    n_ep = mesh.shape["ep"]
    NZ, NX = (8, n_ep // 16) if n_ep >= 32 else (2, n_ep // 4)
    if NZ == 8:
        orders = (
            (0, 6, 1, 2, 4, 5, 3, 7),
            (1, 0, 2, 7, 5, 4, 6, 3),
            (2, 3, 0, 4, 1, 6, 5, 7),
            (3, 2, 1, 6, 4, 7, 0, 5),
            (4, 3, 6, 2, 1, 0, 7, 5),
            (5, 4, 3, 2, 7, 0, 1, 6),
            (6, 4, 0, 3, 2, 1, 5, 7),
            (7, 1, 6, 0, 3, 4, 2, 5),
        )
    else:
        orders = tuple(tuple((n + c) % NZ for c in range(NZ)) for n in range(NZ))
    in_specs = (
        P("ep", "tp"), P("ep", "tp"), P("ep", "tp"), P(None, "tp"), P("tp", None), P("ep", "tp"), P(),
        P("ep", None), P("ep", None), P("ep", None, "tp"), P("ep", None, "tp"), P("ep", "tp", None),
    )
    out_specs = (P(("ep", "tp"), None), P("ep", "tp"))
    return jax.shard_map(
        functools.partial(body, dims=(NZ, NX, orders)),
        mesh=mesh, in_specs=in_specs, out_specs=out_specs, check_vma=False,
    )
```

```python
import functools

import jax
import jax.numpy as jnp
from jax import lax
from jax.experimental import pallas as pl
from jax.experimental.pallas import tpu as pltpu
from jax.sharding import PartitionSpec as P

CAP = 12
TP = 4
BF = jnp.bfloat16
F32 = jnp.float32


def iota(shape, dim):
    return lax.broadcasted_iota(jnp.int32, shape, dim)


def to_message(v, groups):
    h = v.shape[1] // 2
    v0 = v[:, :h].reshape(groups // 2, 8, h)
    v1 = v[:, h:].reshape(groups // 2, 8, h)
    low = iota(v0.shape, 1) < 4
    even = jnp.where(low, v0, pltpu.roll(v1, 4, axis=1))
    odd = jnp.where(low, pltpu.roll(v0, 4, axis=1), v1)
    return even, odd


def from_message(m, groups):
    h = m.shape[2]
    pairs = m.reshape(groups // 2, 2, 8, h)
    even, odd = pairs[:, 0], pairs[:, 1]
    low = iota(even.shape, 1) < 4
    v0 = jnp.where(low, even, pltpu.roll(odd, 4, axis=1))
    v1 = jnp.where(low, pltpu.roll(even, 4, axis=1), odd)
    return v0.reshape(groups * 4, h), v1.reshape(groups * 4, h)


def kernel(
    dims,
    bg_h, cg_h, ci_h, taps_h, mixw, x_h, gain_h, routes_h, rw_h, wg, wu, wd,
    mixed, routed,
    bg, cg, ci, taps, x, gain, routes, rw,
    wg_v, wu_v, wd_v, mw_v, out, G, nrm, PS, R1, FR, ACC, FIN, ret,
    halo, MS, MR1, MF, MACC, XS, XR1, XF, XACC, XO, pick_a, pick_b,
    wsem, halo_s, halo_r, disp_s, disp_r, gd_s, gd_r, gr_s, gr_r,
    r1_s, r1_r, fi_s, fi_r, fa_s, fa_r, back_s, back_r,
    m1_s, m1_r, mi_s, mi_r, ma_s, ma_r, x1_s, x1_r, xi_s, xi_r, xa_s, xa_r, xin_s, xin_r, xo_s, xo_r,
):
    NZ, NX, orders = dims
    S = NX * 2
    H = S // 2
    n_ep = NZ * S
    ntok, DS = x.shape
    h = DS // 2
    rows = S * CAP
    ar = S * 8
    i = lax.axis_index("ep")
    y = lax.axis_index("tp")
    up = (y + 1) & (TP - 1)
    down = (y + 3) & (TP - 1)
    far = (y + 2) & (TP - 1)
    ic = i & 1
    ix = (i >> 1) & (NX - 1)
    iz = i // S
    sides = ((0, up), (1, down))

    def device(dz, dx, dc):
        return ((((iz + dz) & (NZ - 1)) * NX + ((ix + dx) & (NX - 1))) << 1) + ((ic + dc) & 1)

    taken, place = jnp.int32(0), jnp.int32(0)
    for n in range(NZ):
        taken = jnp.where(iz == n, sum(p << 4 * c for c, p in enumerate(orders[n])), taken)
        place = jnp.where(iz == n, sum(orders[e].index(n) << 4 * e for e in range(NZ)), place)

    def remote(src, dst, ssem, rsem, ep=None, tp=None):
        return pltpu.make_async_remote_copy(
            src_ref=src, dst_ref=dst, send_sem=ssem, recv_sem=rsem,
            device_id=(i if ep is None else ep, y if tp is None else tp),
            device_id_type=pl.DeviceIdType.MESH,
        )

    def arrived(ref, sem):
        remote(ref, ref, sem, sem, tp=up).wait_recv()

    def left(ref, sem):
        remote(ref, ref, sem, sem, tp=up).wait_send()

    barrier = pltpu.get_barrier_semaphore()

    def greet(ep, tp):
        pl.semaphore_signal(barrier, inc=1, device_id=(ep, tp), device_id_type=pl.DeviceIdType.MESH)

    for dz in sorted(range(NZ), key=lambda n: -min(n, NZ - n)):
        for r in range(S):
            if dz + r:
                greet(device(dz, r // 2, r % 2), y)
    for _, other in sides:
        greet(i, other)

    loads = [
        pltpu.make_async_copy(src, dst, wsem.at[n])
        for n, (src, dst) in enumerate(
            (
                (routes_h, routes), (x_h, x), (cg_h, cg), (ci_h, ci), (bg_h, bg), (taps_h, taps), (mixw, mw_v),
                (rw_h, rw), (gain_h, gain), (wg.at[0], wg_v), (wu.at[0], wu_v), (wd.at[0], wd_v),
            )
        )
    ]
    for load in loads:
        load.start()

    loads[0].wait()
    e = routes[...]
    dz = (e // S + NZ - iz) & (NZ - 1)
    dx = ((e >> 1) + NX - ix) & (NX - 1)
    dc = (e + ic) & 1
    k = dz * S + dx * 2 + dc
    hot = [iota((n_ep, ntok), 0) == k[q : q + 1] for q in range(2)]
    named = jnp.where(hot[0] | hot[1], 1.0, 0.0).astype(BF)
    before = jnp.where(iota((ntok, ntok), 0) < iota((ntok, ntok), 1), 1.0, 0.0).astype(BF)
    rank = jnp.dot(named, before, preferred_element_type=F32)
    marks = []
    for q in range(2):
        slot = jnp.sum(jnp.where(hot[q], rank, 0.0), axis=0, keepdims=True).astype(jnp.int32)
        kq = k[q : q + 1]
        marks.append(
            (jnp.where(slot < 8, kq * 8 + slot, -1), jnp.where(slot >= 8, kq * 4 + slot - 8, -1))
        )
    ia = iota((n_ep * 8, ntok), 0)
    ib = iota((n_ep * 4, ntok), 0)
    pa = jnp.where((ia == marks[0][0]) | (ia == marks[1][0]), 1.0, 0.0).astype(BF)
    pb = jnp.where((ib == marks[0][1]) | (ib == marks[1][1]), 1.0, 0.0).astype(BF)
    loads[1].wait()
    xv = x[...]
    oa = jnp.dot(pa, xv, preferred_element_type=F32).reshape(n_ep, 8, DS).astype(BF)
    out[:, :, :DS] = oa
    even, odd = to_message(jnp.dot(pb, xv, preferred_element_type=F32), n_ep)
    for p in range(n_ep // 2):
        out[2 * p, :, DS:] = even[p].astype(BF)
        out[2 * p + 1, :, DS:] = odd[p].astype(BF)
    G[0, 0, 0] = out[0]

    for load in loads[2:7]:
        load.wait()
    groups, more = MS.shape[1], XS.shape[1] // 2
    mrows = (groups + more) * 8
    buddy = i + 1 - 2 * ic
    prod = cg[...].astype(F32) * ci[...].astype(F32)
    back1 = pltpu.roll(prod, 1, axis=0)
    back2 = pltpu.roll(prod, 2, axis=0)
    tv = taps[...]
    conv = tv[0:1] * back2 + tv[1:2] * back1 + tv[2:3] * prod
    gated = (bg[...].astype(F32) * conv).astype(BF)
    for q in range(TP):
        product = jnp.dot(gated[q * mrows : (q + 1) * mrows], mw_v[...], preferred_element_type=F32)
        product = product.reshape(groups + more, 8, product.shape[1]).astype(BF)
        if q:
            MS[q] = product[:groups]
        XS[q, pl.ds(0, more)] = product[groups:]

    pl.semaphore_wait(barrier, n_ep - 1 + 2)

    ntail = cg.shape[0] - 8
    tails = [
        remote(ref.at[pl.ds(ntail, 8)], halo.at[q], halo_s.at[q], halo_r.at[q], ep=(i + 1) & (n_ep - 1))
        for q, ref in enumerate((cg, ci))
    ]
    def begin(own, first, last, size, sems, ready):
        half = size // 2
        for d, other in sides:
            keep = (1 - d) * half

            @pl.when(ready(far))
            def _():
                remote(
                    own.at[far, pl.ds(d * half, half)], first.at[d], sems[0].at[d], sems[1].at[d], tp=other
                ).start()

            @pl.when(ready(other))
            def _():
                remote(
                    own.at[other, pl.ds(keep, half)], last.at[d, pl.ds(keep, half)], sems[2].at[d], sems[3].at[d],
                    tp=other,
                ).start()

    m_sems = (m1_s, m1_r, mi_s, mi_r, ma_s, ma_r)
    x_sems = (x1_s, x1_r, xi_s, xi_r, xa_s, xa_r)
    for tail in tails:
        tail.start()
    def dispatch(dz):
        c = (place >> (((iz + dz) & (NZ - 1)) * 4)) & 15 if dz else 0
        for r in range(S):
            if dz + r:
                remote(
                    out.at[dz * S + r], G.at[0, c, r], disp_s, disp_r.at[c], ep=device(dz, r // 2, r % 2)
                ).start()

    dispatch(0)
    begin(MS, MR1, MF, groups, m_sems, lambda q: q > 0)

    handed = [
        remote(XS.at[q, pl.ds(0, more)], XS.at[q, pl.ds(more, more)], xin_s.at[q], xin_r.at[q], ep=buddy)
        for q in range(TP)
    ]

    @pl.when(ic == 0)
    def _():
        for hand in handed:
            hand.start()

    for dz in sorted(range(1, NZ), key=lambda n: min(n, NZ - n)):
        dispatch(dz)

    for tail in tails:
        tail.wait_recv()
    prev = halo[0].astype(F32) * halo[1].astype(F32)
    prev = jnp.where(i > 0, prev, 0.0)
    row = iota((mrows, prod.shape[1]), 0)
    first1 = jnp.where(row == 0, prev[7:8], back1[:mrows])
    first2 = jnp.where(row == 0, prev[6:7], jnp.where(row == 1, prev[7:8], back2[:mrows]))
    conv = tv[0:1] * first2 + tv[1:2] * first1 + tv[2:3] * prod[:mrows]
    gated = (bg[pl.ds(0, mrows), :].astype(F32) * conv).astype(BF)
    product = jnp.dot(gated, mw_v[...], preferred_element_type=F32)
    MS[0] = product.reshape(groups + more, 8, product.shape[1])[:groups].astype(BF)

    def pass_on(own, first, last, added, size, sems):
        half = size // 2
        for d, other in sides:
            part = pl.ds(d * half, half)
            arrived(first.at[d], sems[1].at[d])
            added[d] = (own[other, part].astype(F32) + first[d].astype(F32)).astype(BF)
            remote(added.at[d], last.at[d, part], sems[4].at[d], sems[5].at[d], tp=other).start()

    def summed(own, last, size, sems):
        half = size // 2
        for d in range(2):
            arrived(last.at[d, pl.ds((1 - d) * half, half)], sems[3].at[d])
            arrived(last.at[d, pl.ds(d * half, half)], sems[5].at[d])
        return (own[y].astype(F32) + last[0].astype(F32) + last[1].astype(F32)).astype(BF)

    begin(MS, MR1, MF, groups, m_sems, lambda q: q == 0)

    @pl.when(ic == 1)
    def _():
        for hand in handed:
            hand.wait_recv()
        begin(XS, XR1, XF, 2 * more, x_sems, lambda q: q >= 0)

    loads[7].wait()
    loads[8].wait()
    table = jnp.concatenate(
        [marks[0][0].astype(F32), marks[1][0].astype(F32), marks[0][1].astype(F32), marks[1][1].astype(F32), rw[...]]
        + [jnp.zeros((122, ntok), F32)],
        axis=0,
    )
    cols = jnp.transpose(table)
    ga = iota((ntok, n_ep * 8), 1)
    gb = iota((ntok, n_ep * 4), 1)
    for q in range(2):
        pick_a[q] = jnp.where(ga == cols[:, q : q + 1].astype(jnp.int32), 1.0, 0.0).astype(BF)
        pick_b[q] = jnp.where(gb == cols[:, 2 + q : 3 + q].astype(jnp.int32), 1.0, 0.0).astype(BF)
    share = [cols[:, 4 + q : 5 + q] for q in range(2)]

    def stage_direct(c):
        @pl.when(c == 0)
        def _():
            arrived(G.at[0, 0, pl.ds(1, S - 1)], disp_r.at[0])

        @pl.when(c > 0)
        def _():
            arrived(G.at[0, c], disp_r.at[c])

        for d, other in sides:
            remote(G.at[0, c], G.at[1 + d, c], gd_s.at[d], gd_r.at[d, c], tp=other).start()

    def stage_relay(c):
        for d, other in sides:
            arrived(G.at[1 + d, c], gd_r.at[d, c])
            half = pl.ds(d * H, H)
            remote(G.at[1 + d, c, half], G.at[3, c, half], gr_s.at[d], gr_r.at[d, c], tp=other).start()

    def stage_expert(c):
        @pl.when(c == 0)
        def _():
            for load in loads[9:]:
                load.wait()

        for d in range(2):
            arrived(G.at[3, c, pl.ds(d * H, H)], gr_r.at[d, c])
        owners = (y, down, up, far)
        total = jnp.zeros((S, 8, 1), F32)
        total_b = jnp.zeros((S, 8, 1), F32)
        for n in range(TP):
            g = G[n, c].astype(F32)
            a, b = g[:, :, :DS], g[:, :, DS:]
            total = total + jnp.sum(a * a, axis=2, keepdims=True)
            total_b = total_b + jnp.sum(b * b, axis=2, keepdims=True)
        width = DS * TP
        total_b = total_b + pltpu.roll(total_b, 4, axis=1)
        sa = lax.rsqrt(total / width + 1e-06)
        sb = lax.rsqrt(total_b / width + 1e-06)
        for n, owner in enumerate(owners):
            g = G[n, c].astype(F32)
            gn = gain[owner]
            nrm[owner, pl.ds(0, ar), :] = (g[:, :, :DS] * sa).reshape(ar, DS).astype(F32) * gn
            v0, v1 = from_message(g[:, :, DS:] * sb, S)
            nrm[owner, pl.ds(ar, rows - ar), pl.ds(0, h)] = v0 * gn[:, :h]
            nrm[owner, pl.ds(ar, rows - ar), pl.ds(h, h)] = v1 * gn[:, h:]
        lhs = jnp.concatenate([nrm[n].astype(BF) for n in range(TP)], axis=1)
        gate = jnp.dot(lhs, wg_v[...], preferred_element_type=F32)
        upper = jnp.dot(lhs, wu_v[...], preferred_element_type=F32)
        hidden = (gate / (1.0 + jnp.exp(-gate)) * upper).astype(BF)
        for q in range(TP):
            part = jnp.dot(hidden, wd_v[:, q * DS : (q + 1) * DS], preferred_element_type=F32)
            PS[c, q, :, :, pl.ds(0, DS)] = part[:ar].reshape(S, 8, DS).astype(BF)
            even, odd = to_message(part[ar:], S)
            for p in range(H):
                PS[c, q, 2 * p, :, pl.ds(DS, h)] = even[p].astype(BF)
                PS[c, q, 2 * p + 1, :, pl.ds(DS, h)] = odd[p].astype(BF)
        for d, other in sides:
            half, rest = pl.ds(d * H, H), pl.ds((1 - d) * H, H)
            remote(PS.at[c, far, half], R1.at[d, c], r1_s.at[d], r1_r.at[d, c], tp=other).start()
            remote(PS.at[c, other, rest], FR.at[d, c, rest], fi_s.at[d], fi_r.at[d, c], tp=other).start()

    def stage_add(c):
        for d, other in sides:
            half = pl.ds(d * H, H)
            arrived(R1.at[d, c], r1_r.at[d, c])
            ACC[d, c] = (PS[c, other, half].astype(F32) + R1[d, c].astype(F32)).astype(BF)
            remote(ACC.at[d, c], FR.at[d, c, half], fa_s.at[d], fa_r.at[d, c], tp=other).start()

    def stage_back(c):
        for d in range(2):
            arrived(FR.at[d, c, pl.ds((1 - d) * H, H)], fi_r.at[d, c])
            arrived(FR.at[d, c, pl.ds(d * H, H)], fa_r.at[d, c])
        whole = PS[c, y].astype(F32) + FR[0, c].astype(F32) + FR[1, c].astype(F32)
        FIN[c] = whole.astype(BF)

        @pl.when(c == 0)
        def _():
            ret[0, 0] = FIN[0, 0]

        plane = (taken >> (4 * c)) & 15
        dz = (iz - plane) & (NZ - 1)
        for r in range(S):
            send = remote(
                FIN.at[c, r], ret.at[dz, r], back_s, back_r.at[dz], ep=device(NZ - dz, NX - r // 2, r % 2)
            )
            if r:
                send.start()
            else:
                pl.when(c > 0)(send.start)

    @pl.loop(-3, NZ + 2)
    def _(u):
        @pl.when((u >= -1) & (u < NZ - 1))
        def _():
            stage_relay(u + 1)

        @pl.when(u < NZ - 3)
        def _():
            stage_direct(u + 3)

        @pl.when((u >= 0) & (u < NZ))
        def _():
            stage_expert(u)

        @pl.when((u >= 1) & (u < NZ + 1))
        def _():
            stage_add(u - 1)

        @pl.when(u == NZ)
        def _():
            pass_on(MS, MR1, MF, MACC, groups, m_sems)

            @pl.when(ic == 1)
            def _():
                pass_on(XS, XR1, XF, XACC, 2 * more, x_sems)

        @pl.when(u >= 2)
        def _():
            stage_back(u - 2)

    kept = groups * 8
    mixed[pl.ds(0, kept), :] = summed(MS, MF, groups, m_sems).reshape(kept, -1)
    result = remote(XO.at[0], XO.at[1], xo_s, xo_r, ep=buddy)

    @pl.when(ic == 1)
    def _():
        both = summed(XS, XF, 2 * more, x_sems)
        XO[0] = both[more:]
        result.start()
        mixed[pl.ds(kept, mrows - kept), :] = both[:more].reshape(mrows - kept, -1)

    @pl.when(ic == 0)
    def _():
        result.wait_recv()
        mixed[pl.ds(kept, mrows - kept), :] = XO[1].reshape(mrows - kept, -1)

    arrived(ret.at[0, pl.ds(1, S - 1)], back_r.at[0])
    for c in range(1, NZ):
        arrived(ret.at[c], back_r.at[c])
    back = ret[...].reshape(n_ep, 8, DS + h)
    ra = back[:, :, :DS].reshape(n_ep * 8, DS)
    b0, b1 = from_message(back[:, :, DS:].astype(F32), n_ep)
    rb = jnp.concatenate([b0, b1], axis=1).astype(BF)
    total = jnp.zeros((ntok, DS), F32)
    for q in range(2):
        row = jnp.dot(pick_a[q], ra, preferred_element_type=F32)
        row = row + jnp.dot(pick_b[q], rb, preferred_element_type=F32)
        total = total + row * share[q]
    routed[...] = total.astype(BF)

    for tail in tails:
        tail.wait_send()
    left(out.at[pl.ds(1, n_ep - 1)], disp_s)
    left(out.at[pl.ds(1, n_ep - 1)], back_s)
    for d in range(2):
        left(G.at[0], gd_s.at[d])
        left(R1.at[0], gr_s.at[d])
        left(R1.at[0], r1_s.at[d])
        left(R1.at[0], fi_s.at[d])
        left(R1.at[0], fa_s.at[d])
        left(MR1.at[0], m1_s.at[d])
        left(MR1.at[0], mi_s.at[d])
        left(MR1.at[0], ma_s.at[d])

    @pl.when(ic == 1)
    def _():
        result.wait_send()
        for d in range(2):
            left(XR1.at[0], x1_s.at[d])
            left(XR1.at[0], xi_s.at[d])
            left(XR1.at[0], xa_s.at[d])

    @pl.when(ic == 0)
    def _():
        for hand in handed:
            hand.wait_send()


def write_out(mixed, routed, mixed_out, routed_out, sems):
    copies = [
        pltpu.make_async_copy(mixed, mixed_out, sems.at[0]),
        pltpu.make_async_copy(routed, routed_out, sems.at[1]),
    ]
    for copy in copies:
        copy.start()
    for copy in copies:
        copy.wait()


def body(mix_bgate, mix_cgate, mix_input, conv_taps, mix_out_w, moe_x, moe_gain, routes, route_w, w_gate, w_up, w_down, *, dims):
    NZ, NX, _ = dims
    S = NX * 2
    H = S // 2
    n_ep = NZ * S
    ntok, DS = moe_x.shape
    D = DS * TP
    F = w_gate.shape[2]
    CH = mix_out_w.shape[0]
    ML = DS + DS // 2
    length = mix_input.shape[0]
    mrows = length // TP
    more = mrows // 16
    groups = mrows // 8 - more
    vmem = pl.BlockSpec(memory_space=pltpu.VMEM)
    hbm = pl.BlockSpec(memory_space=pltpu.HBM)
    V = pltpu.VMEM
    dma = pltpu.SemaphoreType.DMA
    results = pl.pallas_call(
        functools.partial(kernel, dims),
        name="step",
        out_shape=(
            V((mrows, D), BF),
            V((ntok, DS), BF),
        ),
        in_specs=[hbm] * 12,
        out_specs=(vmem, vmem),
        scratch_shapes=[
            V((length, CH), BF), V((length, CH), BF), V((length, CH), BF), V((3, CH), F32),
            V((ntok, DS), BF), V((TP, 1, DS), F32), V((2, ntok), jnp.int32), V((2, ntok), F32),
            V((D, F), BF), V((D, F), BF), V((F, D), BF), V((CH, D), BF),
            V((n_ep, 8, ML), BF),
            V((4, NZ, S, 8, ML), BF),
            V((TP, S * CAP, DS), F32),
            V((NZ, TP, S, 8, ML), BF),
            V((2, NZ, H, 8, ML), BF),
            V((2, NZ, S, 8, ML), BF),
            V((2, NZ, H, 8, ML), BF),
            V((NZ, S, 8, ML), BF),
            V((NZ, S, 8, ML), BF),
            V((2, 8, CH), BF),
            V((TP, groups, 8, D), BF),
            V((2, groups // 2, 8, D), BF),
            V((2, groups, 8, D), BF),
            V((2, groups // 2, 8, D), BF),
            V((TP, 2 * more, 8, D), BF),
            V((2, more, 8, D), BF),
            V((2, 2 * more, 8, D), BF),
            V((2, more, 8, D), BF),
            V((2, more, 8, D), BF),
            V((2, ntok, n_ep * 8), BF), V((2, ntok, n_ep * 4), BF),
            dma((12,)), dma((2,)), dma((2,)),
            dma, dma((NZ,)),
            dma((2,)), dma((2, NZ)), dma((2,)), dma((2, NZ)),
            dma((2,)), dma((2, NZ)), dma((2,)), dma((2, NZ)), dma((2,)), dma((2, NZ)),
            dma, dma((NZ,)),
            dma((2,)), dma((2,)), dma((2,)), dma((2,)), dma((2,)), dma((2,)),
            dma((2,)), dma((2,)), dma((2,)), dma((2,)), dma((2,)), dma((2,)),
            dma((TP,)), dma((TP,)), dma, dma,
        ],
        compiler_params=pltpu.CompilerParams(
            collective_id=0, has_side_effects=True, vmem_limit_bytes=67043328 - 2 * 2 * mrows * D - 16384
        ),
    )(
        mix_bgate, mix_cgate, mix_input, conv_taps, mix_out_w, moe_x,
        moe_gain.reshape(TP, 1, DS), routes.T, route_w.T, w_gate, w_up, w_down,
    )
    return pl.pallas_call(
        write_out,
        name="write_out",
        out_shape=tuple(jax.ShapeDtypeStruct(r.shape, BF) for r in results),
        in_specs=[vmem, vmem],
        out_specs=(hbm, hbm),
        scratch_shapes=[dma((2,))],
        compiler_params=pltpu.CompilerParams(vmem_limit_bytes=1024 * 1024),
    )(*results)


def solution(mesh):
    n_ep = mesh.shape["ep"]
    NZ, NX = (8, n_ep // 16) if n_ep >= 32 else (2, n_ep // 4)
    if NZ == 8:
        orders = (
            (0, 1, 2, 3, 4, 5, 6, 7),
            (1, 0, 2, 3, 5, 6, 4, 7),
            (2, 1, 3, 0, 6, 7, 5, 4),
            (3, 2, 1, 0, 7, 6, 5, 4),
            (4, 3, 2, 1, 0, 7, 6, 5),
            (5, 4, 3, 0, 1, 2, 7, 6),
            (6, 7, 0, 1, 2, 3, 4, 5),
            (7, 0, 1, 2, 3, 4, 5, 6),
        )
    else:
        orders = tuple(tuple((n + c) % NZ for c in range(NZ)) for n in range(NZ))
    in_specs = (
        P("ep", "tp"), P("ep", "tp"), P("ep", "tp"), P(None, "tp"), P("tp", None), P("ep", "tp"), P(),
        P("ep", None), P("ep", None), P("ep", None, "tp"), P("ep", None, "tp"), P("ep", "tp", None),
    )
    out_specs = (P(("ep", "tp"), None), P("ep", "tp"))
    return jax.shard_map(
        functools.partial(body, dims=(NZ, NX, orders)),
        mesh=mesh, in_specs=in_specs, out_specs=out_specs, check_vma=False,
    )
```

```python
import functools

import jax
import jax.numpy as jnp
from jax import lax
from jax.experimental import pallas as pl
from jax.experimental.pallas import tpu as pltpu
from jax.sharding import PartitionSpec as P

CAP = 12
TP = 4
BF = jnp.bfloat16
F32 = jnp.float32


def iota(shape, dim):
    return lax.broadcasted_iota(jnp.int32, shape, dim)


def to_message(v, groups):
    h = v.shape[1] // 2
    v0 = v[:, :h].reshape(groups // 2, 8, h)
    v1 = v[:, h:].reshape(groups // 2, 8, h)
    low = iota(v0.shape, 1) < 4
    even = jnp.where(low, v0, pltpu.roll(v1, 4, axis=1))
    odd = jnp.where(low, pltpu.roll(v0, 4, axis=1), v1)
    return even, odd


def from_message(m, groups):
    h = m.shape[2]
    pairs = m.reshape(groups // 2, 2, 8, h)
    even, odd = pairs[:, 0], pairs[:, 1]
    low = iota(even.shape, 1) < 4
    v0 = jnp.where(low, even, pltpu.roll(odd, 4, axis=1))
    v1 = jnp.where(low, pltpu.roll(even, 4, axis=1), odd)
    return v0.reshape(groups * 4, h), v1.reshape(groups * 4, h)


def kernel(
    dims,
    bg_h, cg_h, ci_h, taps_h, mixw, x_h, gain_h, routes_h, rw_h, wg, wu, wd,
    mixed, routed,
    bg, cg, ci, taps, x, gain, routes, rw,
    wg_v, wu_v, wd_v, mw_v, out, G, nrm, PS, R1, FR, ACC, FIN, ret,
    halo, MS, MR1, MF, MACC, XS, XR1, XF, XACC, XO, pick_a, pick_b,
    wsem, halo_s, halo_r, disp_s, disp_r, gd_s, gd_r, gr_s, gr_r,
    r1_s, r1_r, fi_s, fi_r, fa_s, fa_r, back_s, back_r,
    m1_s, m1_r, mi_s, mi_r, ma_s, ma_r, x1_s, x1_r, xi_s, xi_r, xa_s, xa_r, xin_s, xin_r, xo_s, xo_r, news,
):
    NZ, NX, orders = dims
    S = NX * 2
    H = S // 2
    n_ep = NZ * S
    ntok, DS = x.shape
    h = DS // 2
    rows = S * CAP
    ar = S * 8
    i = lax.axis_index("ep")
    y = lax.axis_index("tp")
    up = (y + 1) & (TP - 1)
    down = (y + 3) & (TP - 1)
    far = (y + 2) & (TP - 1)
    ic = i & 1
    ix = (i >> 1) & (NX - 1)
    iz = i // S
    sides = ((0, up), (1, down))

    def device(dz, dx, dc):
        return ((((iz + dz) & (NZ - 1)) * NX + ((ix + dx) & (NX - 1))) << 1) + ((ic + dc) & 1)

    taken, place = jnp.int32(0), jnp.int32(0)
    for n in range(NZ):
        taken = jnp.where(iz == n, sum(p << 4 * c for c, p in enumerate(orders[n])), taken)
        place = jnp.where(iz == n, sum(orders[e].index(n) << 4 * e for e in range(NZ)), place)

    def remote(src, dst, ssem, rsem, ep=None, tp=None):
        return pltpu.make_async_remote_copy(
            src_ref=src, dst_ref=dst, send_sem=ssem, recv_sem=rsem,
            device_id=(i if ep is None else ep, y if tp is None else tp),
            device_id_type=pl.DeviceIdType.MESH,
        )

    def arrived(ref, sem):
        remote(ref, ref, sem, sem, tp=up).wait_recv()

    def left(ref, sem):
        remote(ref, ref, sem, sem, tp=up).wait_send()

    barrier = pltpu.get_barrier_semaphore()

    def greet(ep, tp):
        pl.semaphore_signal(barrier, inc=1, device_id=(ep, tp), device_id_type=pl.DeviceIdType.MESH)

    greet((i + n_ep - 1) & (n_ep - 1), y)
    beside = (device(1, 0, 0), device(NZ - 1, 0, 0))
    for other in beside:
        greet(other, y)
    for r in range(1, S):
        greet(device(0, r // 2, r % 2), y)
    for _, other in sides:
        greet(i, other)

    def tell(n):
        for d, other in enumerate(beside):
            pl.semaphore_signal(
                news.at[n, d], inc=1, device_id=(other, y), device_id_type=pl.DeviceIdType.MESH
            )

    def reach(n):
        for d in range(2):
            pl.semaphore_wait(news.at[n, d], 1)
        if n + 1 < NZ // 2:
            tell(n + 1)
        for dz in sorted({n + 1, NZ - n - 1}):
            dispatch(dz)

    loads = [
        pltpu.make_async_copy(src, dst, wsem.at[n])
        for n, (src, dst) in enumerate(
            (
                (routes_h, routes), (x_h, x), (cg_h, cg), (ci_h, ci), (bg_h, bg), (taps_h, taps), (mixw, mw_v),
                (rw_h, rw), (gain_h, gain), (wg.at[0], wg_v), (wu.at[0], wu_v), (wd.at[0], wd_v),
            )
        )
    ]
    for load in loads:
        load.start()

    loads[0].wait()
    e = routes[...]
    dz = (e // S + NZ - iz) & (NZ - 1)
    dx = ((e >> 1) + NX - ix) & (NX - 1)
    dc = (e + ic) & 1
    k = dz * S + dx * 2 + dc
    hot = [iota((n_ep, ntok), 0) == k[q : q + 1] for q in range(2)]
    named = jnp.where(hot[0] | hot[1], 1.0, 0.0).astype(BF)
    before = jnp.where(iota((ntok, ntok), 0) < iota((ntok, ntok), 1), 1.0, 0.0).astype(BF)
    rank = jnp.dot(named, before, preferred_element_type=F32)
    marks = []
    for q in range(2):
        slot = jnp.sum(jnp.where(hot[q], rank, 0.0), axis=0, keepdims=True).astype(jnp.int32)
        kq = k[q : q + 1]
        marks.append(
            (jnp.where(slot < 8, kq * 8 + slot, -1), jnp.where(slot >= 8, kq * 4 + slot - 8, -1))
        )
    ia = iota((n_ep * 8, ntok), 0)
    ib = iota((n_ep * 4, ntok), 0)
    pa = jnp.where((ia == marks[0][0]) | (ia == marks[1][0]), 1.0, 0.0).astype(BF)
    pb = jnp.where((ib == marks[0][1]) | (ib == marks[1][1]), 1.0, 0.0).astype(BF)
    loads[1].wait()
    xv = x[...]
    oa = jnp.dot(pa, xv, preferred_element_type=F32).reshape(n_ep, 8, DS).astype(BF)
    out[:, :, :DS] = oa
    even, odd = to_message(jnp.dot(pb, xv, preferred_element_type=F32), n_ep)
    for p in range(n_ep // 2):
        out[2 * p, :, DS:] = even[p].astype(BF)
        out[2 * p + 1, :, DS:] = odd[p].astype(BF)
    G[0, 0, 0] = out[0]

    for load in loads[2:7]:
        load.wait()
    groups, more = MS.shape[1], XS.shape[1] // 2
    mrows = (groups + more) * 8
    buddy = i + 1 - 2 * ic
    prod = cg[...].astype(F32) * ci[...].astype(F32)
    back1 = pltpu.roll(prod, 1, axis=0)
    back2 = pltpu.roll(prod, 2, axis=0)
    tv = taps[...]
    conv = tv[0:1] * back2 + tv[1:2] * back1 + tv[2:3] * prod
    gated = (bg[...].astype(F32) * conv).astype(BF)
    for q in range(TP):
        product = jnp.dot(gated[q * mrows : (q + 1) * mrows], mw_v[...], preferred_element_type=F32)
        product = product.reshape(groups + more, 8, product.shape[1]).astype(BF)
        if q:
            MS[q] = product[:groups]
        XS[q, pl.ds(0, more)] = product[groups:]

    pl.semaphore_wait(barrier, S - 1 + 5)
    tell(0)

    ntail = cg.shape[0] - 8
    tails = [
        remote(ref.at[pl.ds(ntail, 8)], halo.at[q], halo_s.at[q], halo_r.at[q], ep=(i + 1) & (n_ep - 1))
        for q, ref in enumerate((cg, ci))
    ]
    def begin(own, first, last, size, sems, ready):
        half = size // 2
        for d, other in sides:
            keep = (1 - d) * half

            @pl.when(ready(far))
            def _():
                remote(
                    own.at[far, pl.ds(d * half, half)], first.at[d], sems[0].at[d], sems[1].at[d], tp=other
                ).start()

            @pl.when(ready(other))
            def _():
                remote(
                    own.at[other, pl.ds(keep, half)], last.at[d, pl.ds(keep, half)], sems[2].at[d], sems[3].at[d],
                    tp=other,
                ).start()

    m_sems = (m1_s, m1_r, mi_s, mi_r, ma_s, ma_r)
    x_sems = (x1_s, x1_r, xi_s, xi_r, xa_s, xa_r)
    for tail in tails:
        tail.start()
    def dispatch(dz):
        c = (place >> (((iz + dz) & (NZ - 1)) * 4)) & 15 if dz else 0
        for r in range(S):
            if dz + r:
                remote(
                    out.at[dz * S + r], G.at[0, c, r], disp_s, disp_r.at[c], ep=device(dz, r // 2, r % 2)
                ).start()

    dispatch(0)
    begin(MS, MR1, MF, groups, m_sems, lambda q: q > 0)

    handed = [
        remote(XS.at[q, pl.ds(0, more)], XS.at[q, pl.ds(more, more)], xin_s.at[q], xin_r.at[q], ep=buddy)
        for q in range(TP)
    ]

    @pl.when(ic == 0)
    def _():
        for hand in handed:
            hand.start()

    reach(0)
    for tail in tails:
        tail.wait_recv()
    prev = halo[0].astype(F32) * halo[1].astype(F32)
    prev = jnp.where(i > 0, prev, 0.0)
    row = iota((mrows, prod.shape[1]), 0)
    first1 = jnp.where(row == 0, prev[7:8], back1[:mrows])
    first2 = jnp.where(row == 0, prev[6:7], jnp.where(row == 1, prev[7:8], back2[:mrows]))
    conv = tv[0:1] * first2 + tv[1:2] * first1 + tv[2:3] * prod[:mrows]
    gated = (bg[pl.ds(0, mrows), :].astype(F32) * conv).astype(BF)
    product = jnp.dot(gated, mw_v[...], preferred_element_type=F32)
    MS[0] = product.reshape(groups + more, 8, product.shape[1])[:groups].astype(BF)

    def pass_on(own, first, last, added, size, sems):
        half = size // 2
        for d, other in sides:
            part = pl.ds(d * half, half)
            arrived(first.at[d], sems[1].at[d])
            added[d] = (own[other, part].astype(F32) + first[d].astype(F32)).astype(BF)
            remote(added.at[d], last.at[d, part], sems[4].at[d], sems[5].at[d], tp=other).start()

    def summed(own, last, size, sems):
        half = size // 2
        for d in range(2):
            arrived(last.at[d, pl.ds((1 - d) * half, half)], sems[3].at[d])
            arrived(last.at[d, pl.ds(d * half, half)], sems[5].at[d])
        return (own[y].astype(F32) + last[0].astype(F32) + last[1].astype(F32)).astype(BF)

    begin(MS, MR1, MF, groups, m_sems, lambda q: q == 0)
    if NZ > 2:
        reach(1)

    @pl.when(ic == 1)
    def _():
        for hand in handed:
            hand.wait_recv()
        begin(XS, XR1, XF, 2 * more, x_sems, lambda q: q >= 0)

    if NZ > 4:
        reach(2)

    loads[7].wait()
    loads[8].wait()
    table = jnp.concatenate(
        [marks[0][0].astype(F32), marks[1][0].astype(F32), marks[0][1].astype(F32), marks[1][1].astype(F32), rw[...]]
        + [jnp.zeros((122, ntok), F32)],
        axis=0,
    )
    cols = jnp.transpose(table)
    ga = iota((ntok, n_ep * 8), 1)
    gb = iota((ntok, n_ep * 4), 1)
    for q in range(2):
        pick_a[q] = jnp.where(ga == cols[:, q : q + 1].astype(jnp.int32), 1.0, 0.0).astype(BF)
        pick_b[q] = jnp.where(gb == cols[:, 2 + q : 3 + q].astype(jnp.int32), 1.0, 0.0).astype(BF)
    share = [cols[:, 4 + q : 5 + q] for q in range(2)]

    if NZ > 6:
        reach(3)

    def stage_direct(c):
        @pl.when(c == 0)
        def _():
            arrived(G.at[0, 0, pl.ds(1, S - 1)], disp_r.at[0])

        @pl.when(c > 0)
        def _():
            arrived(G.at[0, c], disp_r.at[c])

        for d, other in sides:
            remote(G.at[0, c], G.at[1 + d, c], gd_s.at[d], gd_r.at[d, c], tp=other).start()

    def stage_relay(c):
        for d, other in sides:
            arrived(G.at[1 + d, c], gd_r.at[d, c])
            half = pl.ds(d * H, H)
            remote(G.at[1 + d, c, half], G.at[3, c, half], gr_s.at[d], gr_r.at[d, c], tp=other).start()

    def stage_expert(c):
        @pl.when(c == 0)
        def _():
            for load in loads[9:]:
                load.wait()

        for d in range(2):
            arrived(G.at[3, c, pl.ds(d * H, H)], gr_r.at[d, c])
        owners = (y, down, up, far)
        total = jnp.zeros((S, 8, 1), F32)
        total_b = jnp.zeros((S, 8, 1), F32)
        for n in range(TP):
            g = G[n, c].astype(F32)
            a, b = g[:, :, :DS], g[:, :, DS:]
            total = total + jnp.sum(a * a, axis=2, keepdims=True)
            total_b = total_b + jnp.sum(b * b, axis=2, keepdims=True)
        width = DS * TP
        total_b = total_b + pltpu.roll(total_b, 4, axis=1)
        sa = lax.rsqrt(total / width + 1e-06)
        sb = lax.rsqrt(total_b / width + 1e-06)
        for n, owner in enumerate(owners):
            g = G[n, c].astype(F32)
            gn = gain[owner]
            nrm[owner, pl.ds(0, ar), :] = (g[:, :, :DS] * sa).reshape(ar, DS).astype(F32) * gn
            v0, v1 = from_message(g[:, :, DS:] * sb, S)
            nrm[owner, pl.ds(ar, rows - ar), pl.ds(0, h)] = v0 * gn[:, :h]
            nrm[owner, pl.ds(ar, rows - ar), pl.ds(h, h)] = v1 * gn[:, h:]
        lhs = jnp.concatenate([nrm[n].astype(BF) for n in range(TP)], axis=1)
        gate = jnp.dot(lhs, wg_v[...], preferred_element_type=F32)
        upper = jnp.dot(lhs, wu_v[...], preferred_element_type=F32)
        hidden = (gate / (1.0 + jnp.exp(-gate)) * upper).astype(BF)
        for q in range(TP):
            part = jnp.dot(hidden, wd_v[:, q * DS : (q + 1) * DS], preferred_element_type=F32)
            PS[c, q, :, :, pl.ds(0, DS)] = part[:ar].reshape(S, 8, DS).astype(BF)
            even, odd = to_message(part[ar:], S)
            for p in range(H):
                PS[c, q, 2 * p, :, pl.ds(DS, h)] = even[p].astype(BF)
                PS[c, q, 2 * p + 1, :, pl.ds(DS, h)] = odd[p].astype(BF)
        for d, other in sides:
            half, rest = pl.ds(d * H, H), pl.ds((1 - d) * H, H)
            remote(PS.at[c, far, half], R1.at[d, c], r1_s.at[d], r1_r.at[d, c], tp=other).start()
            remote(PS.at[c, other, rest], FR.at[d, c, rest], fi_s.at[d], fi_r.at[d, c], tp=other).start()

    def stage_add(c):
        for d, other in sides:
            half = pl.ds(d * H, H)
            arrived(R1.at[d, c], r1_r.at[d, c])
            ACC[d, c] = (PS[c, other, half].astype(F32) + R1[d, c].astype(F32)).astype(BF)
            remote(ACC.at[d, c], FR.at[d, c, half], fa_s.at[d], fa_r.at[d, c], tp=other).start()

    def stage_back(c):
        for d in range(2):
            arrived(FR.at[d, c, pl.ds((1 - d) * H, H)], fi_r.at[d, c])
            arrived(FR.at[d, c, pl.ds(d * H, H)], fa_r.at[d, c])
        whole = PS[c, y].astype(F32) + FR[0, c].astype(F32) + FR[1, c].astype(F32)
        FIN[c] = whole.astype(BF)

        @pl.when(c == 0)
        def _():
            ret[0, 0] = FIN[0, 0]

        plane = (taken >> (4 * c)) & 15
        dz = (iz - plane) & (NZ - 1)
        for r in range(S):
            send = remote(
                FIN.at[c, r], ret.at[dz, r], back_s, back_r.at[dz], ep=device(NZ - dz, NX - r // 2, r % 2)
            )
            if r:
                send.start()
            else:
                pl.when(c > 0)(send.start)

    @pl.loop(-3, NZ + 2)
    def _(u):
        @pl.when((u >= -1) & (u < NZ - 1))
        def _():
            stage_relay(u + 1)

        @pl.when(u < NZ - 3)
        def _():
            stage_direct(u + 3)

        @pl.when((u >= 0) & (u < NZ))
        def _():
            stage_expert(u)

        @pl.when((u >= 1) & (u < NZ + 1))
        def _():
            stage_add(u - 1)

        @pl.when(u == NZ)
        def _():
            pass_on(MS, MR1, MF, MACC, groups, m_sems)

            @pl.when(ic == 1)
            def _():
                pass_on(XS, XR1, XF, XACC, 2 * more, x_sems)

        @pl.when(u >= 2)
        def _():
            stage_back(u - 2)

    kept = groups * 8
    mixed[pl.ds(0, kept), :] = summed(MS, MF, groups, m_sems).reshape(kept, -1)
    result = remote(XO.at[0], XO.at[1], xo_s, xo_r, ep=buddy)

    @pl.when(ic == 1)
    def _():
        both = summed(XS, XF, 2 * more, x_sems)
        XO[0] = both[more:]
        result.start()
        mixed[pl.ds(kept, mrows - kept), :] = both[:more].reshape(mrows - kept, -1)

    @pl.when(ic == 0)
    def _():
        result.wait_recv()
        mixed[pl.ds(kept, mrows - kept), :] = XO[1].reshape(mrows - kept, -1)

    arrived(ret.at[0, pl.ds(1, S - 1)], back_r.at[0])
    for c in range(1, NZ):
        arrived(ret.at[c], back_r.at[c])
    back = ret[...].reshape(n_ep, 8, DS + h)
    ra = back[:, :, :DS].reshape(n_ep * 8, DS)
    b0, b1 = from_message(back[:, :, DS:].astype(F32), n_ep)
    rb = jnp.concatenate([b0, b1], axis=1).astype(BF)
    total = jnp.zeros((ntok, DS), F32)
    for q in range(2):
        row = jnp.dot(pick_a[q], ra, preferred_element_type=F32)
        row = row + jnp.dot(pick_b[q], rb, preferred_element_type=F32)
        total = total + row * share[q]
    routed[...] = total.astype(BF)

    for tail in tails:
        tail.wait_send()
    left(out.at[pl.ds(1, n_ep - 1)], disp_s)
    left(out.at[pl.ds(1, n_ep - 1)], back_s)
    for d in range(2):
        left(G.at[0], gd_s.at[d])
        left(R1.at[0], gr_s.at[d])
        left(R1.at[0], r1_s.at[d])
        left(R1.at[0], fi_s.at[d])
        left(R1.at[0], fa_s.at[d])
        left(MR1.at[0], m1_s.at[d])
        left(MR1.at[0], mi_s.at[d])
        left(MR1.at[0], ma_s.at[d])

    @pl.when(ic == 1)
    def _():
        result.wait_send()
        for d in range(2):
            left(XR1.at[0], x1_s.at[d])
            left(XR1.at[0], xi_s.at[d])
            left(XR1.at[0], xa_s.at[d])

    @pl.when(ic == 0)
    def _():
        for hand in handed:
            hand.wait_send()


def write_out(mixed, routed, mixed_out, routed_out, sems):
    copies = [
        pltpu.make_async_copy(mixed, mixed_out, sems.at[0]),
        pltpu.make_async_copy(routed, routed_out, sems.at[1]),
    ]
    for copy in copies:
        copy.start()
    for copy in copies:
        copy.wait()


def body(mix_bgate, mix_cgate, mix_input, conv_taps, mix_out_w, moe_x, moe_gain, routes, route_w, w_gate, w_up, w_down, *, dims):
    NZ, NX, _ = dims
    S = NX * 2
    H = S // 2
    n_ep = NZ * S
    ntok, DS = moe_x.shape
    D = DS * TP
    F = w_gate.shape[2]
    CH = mix_out_w.shape[0]
    ML = DS + DS // 2
    length = mix_input.shape[0]
    mrows = length // TP
    more = mrows // 16
    groups = mrows // 8 - more
    vmem = pl.BlockSpec(memory_space=pltpu.VMEM)
    hbm = pl.BlockSpec(memory_space=pltpu.HBM)
    V = pltpu.VMEM
    dma = pltpu.SemaphoreType.DMA
    results = pl.pallas_call(
        functools.partial(kernel, dims),
        name="step",
        out_shape=(
            V((mrows, D), BF),
            V((ntok, DS), BF),
        ),
        in_specs=[hbm] * 12,
        out_specs=(vmem, vmem),
        scratch_shapes=[
            V((length, CH), BF), V((length, CH), BF), V((length, CH), BF), V((3, CH), F32),
            V((ntok, DS), BF), V((TP, 1, DS), F32), V((2, ntok), jnp.int32), V((2, ntok), F32),
            V((D, F), BF), V((D, F), BF), V((F, D), BF), V((CH, D), BF),
            V((n_ep, 8, ML), BF),
            V((4, NZ, S, 8, ML), BF),
            V((TP, S * CAP, DS), F32),
            V((NZ, TP, S, 8, ML), BF),
            V((2, NZ, H, 8, ML), BF),
            V((2, NZ, S, 8, ML), BF),
            V((2, NZ, H, 8, ML), BF),
            V((NZ, S, 8, ML), BF),
            V((NZ, S, 8, ML), BF),
            V((2, 8, CH), BF),
            V((TP, groups, 8, D), BF),
            V((2, groups // 2, 8, D), BF),
            V((2, groups, 8, D), BF),
            V((2, groups // 2, 8, D), BF),
            V((TP, 2 * more, 8, D), BF),
            V((2, more, 8, D), BF),
            V((2, 2 * more, 8, D), BF),
            V((2, more, 8, D), BF),
            V((2, more, 8, D), BF),
            V((2, ntok, n_ep * 8), BF), V((2, ntok, n_ep * 4), BF),
            dma((12,)), dma((2,)), dma((2,)),
            dma, dma((NZ,)),
            dma((2,)), dma((2, NZ)), dma((2,)), dma((2, NZ)),
            dma((2,)), dma((2, NZ)), dma((2,)), dma((2, NZ)), dma((2,)), dma((2, NZ)),
            dma, dma((NZ,)),
            dma((2,)), dma((2,)), dma((2,)), dma((2,)), dma((2,)), dma((2,)),
            dma((2,)), dma((2,)), dma((2,)), dma((2,)), dma((2,)), dma((2,)),
            dma((TP,)), dma((TP,)), dma, dma, pltpu.SemaphoreType.REGULAR((NZ // 2, 2)),
        ],
        compiler_params=pltpu.CompilerParams(
            collective_id=0, has_side_effects=True, vmem_limit_bytes=67043328 - 2 * 2 * mrows * D - 16384
        ),
    )(
        mix_bgate, mix_cgate, mix_input, conv_taps, mix_out_w, moe_x,
        moe_gain.reshape(TP, 1, DS), routes.T, route_w.T, w_gate, w_up, w_down,
    )
    return pl.pallas_call(
        write_out,
        name="write_out",
        out_shape=tuple(jax.ShapeDtypeStruct(r.shape, BF) for r in results),
        in_specs=[vmem, vmem],
        out_specs=(hbm, hbm),
        scratch_shapes=[dma((2,))],
        compiler_params=pltpu.CompilerParams(vmem_limit_bytes=1024 * 1024),
    )(*results)


def solution(mesh):
    n_ep = mesh.shape["ep"]
    NZ, NX = (8, n_ep // 16) if n_ep >= 32 else (2, n_ep // 4)
    if NZ == 8:
        orders = (
            (0, 1, 2, 3, 4, 5, 6, 7),
            (1, 0, 2, 3, 5, 6, 4, 7),
            (2, 1, 3, 0, 6, 7, 5, 4),
            (3, 2, 1, 0, 7, 6, 5, 4),
            (4, 3, 2, 1, 0, 7, 6, 5),
            (5, 4, 3, 0, 1, 2, 7, 6),
            (6, 7, 0, 1, 2, 3, 4, 5),
            (7, 0, 1, 2, 3, 4, 5, 6),
        )
    else:
        orders = tuple(tuple((n + c) % NZ for c in range(NZ)) for n in range(NZ))
    in_specs = (
        P("ep", "tp"), P("ep", "tp"), P("ep", "tp"), P(None, "tp"), P("tp", None), P("ep", "tp"), P(),
        P("ep", None), P("ep", None), P("ep", None, "tp"), P("ep", None, "tp"), P("ep", "tp", None),
    )
    out_specs = (P(("ep", "tp"), None), P("ep", "tp"))
    return jax.shard_map(
        functools.partial(body, dims=(NZ, NX, orders)),
        mesh=mesh, in_specs=in_specs, out_specs=out_specs, check_vma=False,
    )
```

```python
import functools

import jax
import jax.numpy as jnp
from jax import lax
from jax.experimental import pallas as pl
from jax.experimental.pallas import tpu as pltpu
from jax.sharding import PartitionSpec as P

CAP = 12
TP = 4
BF = jnp.bfloat16
F32 = jnp.float32


def iota(shape, dim):
    return lax.broadcasted_iota(jnp.int32, shape, dim)


def to_message(v, groups):
    h = v.shape[1] // 2
    v0 = v[:, :h].reshape(groups // 2, 8, h)
    v1 = v[:, h:].reshape(groups // 2, 8, h)
    low = iota(v0.shape, 1) < 4
    even = jnp.where(low, v0, pltpu.roll(v1, 4, axis=1))
    odd = jnp.where(low, pltpu.roll(v0, 4, axis=1), v1)
    return even, odd


def from_message(m, groups):
    h = m.shape[2]
    pairs = m.reshape(groups // 2, 2, 8, h)
    even, odd = pairs[:, 0], pairs[:, 1]
    low = iota(even.shape, 1) < 4
    v0 = jnp.where(low, even, pltpu.roll(odd, 4, axis=1))
    v1 = jnp.where(low, pltpu.roll(even, 4, axis=1), odd)
    return v0.reshape(groups * 4, h), v1.reshape(groups * 4, h)


def kernel(
    dims,
    bg_h, cg_h, ci_h, taps_h, mixw, x_h, gain_h, routes_h, rw_h, wg, wu, wd,
    mixed, routed,
    bg, cg, ci, taps, x, gain, routes, rw,
    wg_v, wu_v, wd_v, mw_v, out, G, nrm, PS, R1, FR, ACC, FIN, ret,
    halo, MS, MR1, MF, MACC, XS, XR1, XF, XACC, XO, pick_a, pick_b,
    wsem, halo_s, halo_r, disp_s, disp_r, gd_s, gd_r, gr_s, gr_r,
    r1_s, r1_r, fi_s, fi_r, fa_s, fa_r, back_s, back_r,
    m1_s, m1_r, mi_s, mi_r, ma_s, ma_r, x1_s, x1_r, xi_s, xi_r, xa_s, xa_r, xin_s, xin_r, xo_s, xo_r, news,
):
    NZ, NX, orders = dims
    S = NX * 2
    H = S // 2
    n_ep = NZ * S
    ntok, DS = x.shape
    h = DS // 2
    rows = S * CAP
    ar = S * 8
    i = lax.axis_index("ep")
    y = lax.axis_index("tp")
    up = (y + 1) & (TP - 1)
    down = (y + 3) & (TP - 1)
    far = (y + 2) & (TP - 1)
    ic = i & 1
    ix = (i >> 1) & (NX - 1)
    iz = i // S
    sides = ((0, up), (1, down))

    def device(dz, dx, dc):
        return ((((iz + dz) & (NZ - 1)) * NX + ((ix + dx) & (NX - 1))) << 1) + ((ic + dc) & 1)

    taken, place = jnp.int32(0), jnp.int32(0)
    for n in range(NZ):
        taken = jnp.where(iz == n, sum(p << 4 * c for c, p in enumerate(orders[n])), taken)
        place = jnp.where(iz == n, sum(orders[e].index(n) << 4 * e for e in range(NZ)), place)

    def remote(src, dst, ssem, rsem, ep=None, tp=None):
        return pltpu.make_async_remote_copy(
            src_ref=src, dst_ref=dst, send_sem=ssem, recv_sem=rsem,
            device_id=(i if ep is None else ep, y if tp is None else tp),
            device_id_type=pl.DeviceIdType.MESH,
        )

    def arrived(ref, sem):
        remote(ref, ref, sem, sem, tp=up).wait_recv()

    def left(ref, sem):
        remote(ref, ref, sem, sem, tp=up).wait_send()

    barrier = pltpu.get_barrier_semaphore()

    def greet(ep, tp):
        pl.semaphore_signal(barrier, inc=1, device_id=(ep, tp), device_id_type=pl.DeviceIdType.MESH)

    greet((i + n_ep - 1) & (n_ep - 1), y)
    beside = (device(1, 0, 0), device(NZ - 1, 0, 0))
    for other in beside:
        greet(other, y)
    for r in range(1, S):
        greet(device(0, r // 2, r % 2), y)
    for _, other in sides:
        greet(i, other)

    def tell(n):
        for d, other in enumerate(beside):
            pl.semaphore_signal(
                news.at[n, d], inc=1, device_id=(other, y), device_id_type=pl.DeviceIdType.MESH
            )

    def reach(n):
        for d in range(2):
            pl.semaphore_wait(news.at[n, d], 1)
        if n + 1 < NZ // 2:
            tell(n + 1)
        for dz in sorted({n + 1, NZ - n - 1}):
            dispatch(dz)

    loads = [
        pltpu.make_async_copy(src, dst, wsem.at[n])
        for n, (src, dst) in enumerate(
            (
                (routes_h, routes), (x_h, x), (cg_h, cg), (ci_h, ci), (bg_h, bg), (taps_h, taps), (mixw, mw_v),
                (rw_h, rw), (gain_h, gain), (wg.at[0], wg_v), (wu.at[0], wu_v), (wd.at[0], wd_v),
            )
        )
    ]
    for load in loads:
        load.start()

    loads[0].wait()
    e = routes[...]
    dz = (e // S + NZ - iz) & (NZ - 1)
    dx = ((e >> 1) + NX - ix) & (NX - 1)
    dc = (e + ic) & 1
    k = dz * S + dx * 2 + dc
    hot = [iota((n_ep, ntok), 0) == k[q : q + 1] for q in range(2)]
    named = jnp.where(hot[0] | hot[1], 1.0, 0.0).astype(BF)
    before = jnp.where(iota((ntok, ntok), 0) < iota((ntok, ntok), 1), 1.0, 0.0).astype(BF)
    rank = jnp.dot(named, before, preferred_element_type=F32)
    marks = []
    for q in range(2):
        slot = jnp.sum(jnp.where(hot[q], rank, 0.0), axis=0, keepdims=True).astype(jnp.int32)
        kq = k[q : q + 1]
        marks.append(
            (jnp.where(slot < 8, kq * 8 + slot, -1), jnp.where(slot >= 8, kq * 4 + slot - 8, -1))
        )
    ia = iota((n_ep * 8, ntok), 0)
    ib = iota((n_ep * 4, ntok), 0)
    pa = jnp.where((ia == marks[0][0]) | (ia == marks[1][0]), 1.0, 0.0).astype(BF)
    pb = jnp.where((ib == marks[0][1]) | (ib == marks[1][1]), 1.0, 0.0).astype(BF)
    loads[1].wait()
    xv = x[...]
    oa = jnp.dot(pa, xv, preferred_element_type=F32).reshape(n_ep, 8, DS).astype(BF)
    out[:, :, :DS] = oa
    even, odd = to_message(jnp.dot(pb, xv, preferred_element_type=F32), n_ep)
    for p in range(n_ep // 2):
        out[2 * p, :, DS:] = even[p].astype(BF)
        out[2 * p + 1, :, DS:] = odd[p].astype(BF)
    G[0, 0, 0] = out[0]

    for load in loads[2:7]:
        load.wait()
    groups, more = MS.shape[1], XS.shape[1] // 2
    mrows = (groups + more) * 8
    buddy = i + 1 - 2 * ic
    prod = cg[...].astype(F32) * ci[...].astype(F32)
    back1 = pltpu.roll(prod, 1, axis=0)
    back2 = pltpu.roll(prod, 2, axis=0)
    tv = taps[...]
    conv = tv[0:1] * back2 + tv[1:2] * back1 + tv[2:3] * prod
    gated = (bg[...].astype(F32) * conv).astype(BF)
    for q in range(TP):
        product = jnp.dot(gated[q * mrows : (q + 1) * mrows], mw_v[...], preferred_element_type=F32)
        product = product.reshape(groups + more, 8, product.shape[1]).astype(BF)
        if q:
            MS[q] = product[:groups]
        XS[q, pl.ds(0, more)] = product[groups:]

    pl.semaphore_wait(barrier, S - 1 + 5)
    tell(0)

    ntail = cg.shape[0] - 8
    tails = [
        remote(ref.at[pl.ds(ntail, 8)], halo.at[q], halo_s.at[q], halo_r.at[q], ep=(i + 1) & (n_ep - 1))
        for q, ref in enumerate((cg, ci))
    ]
    def begin(own, first, last, size, sems, ready):
        half = size // 2
        for d, other in sides:
            keep = (1 - d) * half

            @pl.when(ready(far))
            def _():
                remote(
                    own.at[far, pl.ds(d * half, half)], first.at[d], sems[0].at[d], sems[1].at[d], tp=other
                ).start()

            @pl.when(ready(other))
            def _():
                remote(
                    own.at[other, pl.ds(keep, half)], last.at[d, pl.ds(keep, half)], sems[2].at[d], sems[3].at[d],
                    tp=other,
                ).start()

    m_sems = (m1_s, m1_r, mi_s, mi_r, ma_s, ma_r)
    x_sems = (x1_s, x1_r, xi_s, xi_r, xa_s, xa_r)
    for tail in tails:
        tail.start()
    def dispatch(dz):
        c = (place >> (((iz + dz) & (NZ - 1)) * 4)) & 15 if dz else 0
        for r in range(S):
            if dz + r:
                remote(
                    out.at[dz * S + r], G.at[0, c, r], disp_s, disp_r.at[c], ep=device(dz, r // 2, r % 2)
                ).start()

    dispatch(0)
    begin(MS, MR1, MF, groups, m_sems, lambda q: q > 0)

    handed = [
        remote(XS.at[q, pl.ds(0, more)], XS.at[q, pl.ds(more, more)], xin_s.at[q], xin_r.at[q], ep=buddy)
        for q in range(TP)
    ]

    @pl.when(ic == 0)
    def _():
        for hand in handed:
            hand.start()

    reach(0)
    for tail in tails:
        tail.wait_recv()
    prev = halo[0].astype(F32) * halo[1].astype(F32)
    prev = jnp.where(i > 0, prev, 0.0)
    row = iota((mrows, prod.shape[1]), 0)
    first1 = jnp.where(row == 0, prev[7:8], back1[:mrows])
    first2 = jnp.where(row == 0, prev[6:7], jnp.where(row == 1, prev[7:8], back2[:mrows]))
    conv = tv[0:1] * first2 + tv[1:2] * first1 + tv[2:3] * prod[:mrows]
    gated = (bg[pl.ds(0, mrows), :].astype(F32) * conv).astype(BF)
    product = jnp.dot(gated, mw_v[...], preferred_element_type=F32)
    MS[0] = product.reshape(groups + more, 8, product.shape[1])[:groups].astype(BF)

    def pass_on(own, first, last, added, size, sems):
        half = size // 2
        for d, other in sides:
            part = pl.ds(d * half, half)
            arrived(first.at[d], sems[1].at[d])
            added[d] = (own[other, part].astype(F32) + first[d].astype(F32)).astype(BF)
            remote(added.at[d], last.at[d, part], sems[4].at[d], sems[5].at[d], tp=other).start()

    def summed(own, last, size, sems):
        half = size // 2
        for d in range(2):
            arrived(last.at[d, pl.ds((1 - d) * half, half)], sems[3].at[d])
            arrived(last.at[d, pl.ds(d * half, half)], sems[5].at[d])
        return (own[y].astype(F32) + last[0].astype(F32) + last[1].astype(F32)).astype(BF)

    begin(MS, MR1, MF, groups, m_sems, lambda q: q == 0)
    if NZ > 2:
        reach(1)

    @pl.when(ic == 1)
    def _():
        for hand in handed:
            hand.wait_recv()
        begin(XS, XR1, XF, 2 * more, x_sems, lambda q: q >= 0)

    if NZ > 4:
        reach(2)

    loads[7].wait()
    loads[8].wait()
    table = jnp.concatenate(
        [marks[0][0].astype(F32), marks[1][0].astype(F32), marks[0][1].astype(F32), marks[1][1].astype(F32), rw[...]]
        + [jnp.zeros((122, ntok), F32)],
        axis=0,
    )
    cols = jnp.transpose(table)
    ga = iota((ntok, n_ep * 8), 1)
    gb = iota((ntok, n_ep * 4), 1)
    for q in range(2):
        pick_a[q] = jnp.where(ga == cols[:, q : q + 1].astype(jnp.int32), 1.0, 0.0).astype(BF)
        pick_b[q] = jnp.where(gb == cols[:, 2 + q : 3 + q].astype(jnp.int32), 1.0, 0.0).astype(BF)
    share = [cols[:, 4 + q : 5 + q] for q in range(2)]

    def stage_direct(c):
        @pl.when(c == 0)
        def _():
            arrived(G.at[0, 0, pl.ds(1, S - 1)], disp_r.at[0])

        @pl.when(c > 0)
        def _():
            arrived(G.at[0, c], disp_r.at[c])

        for d, other in sides:
            remote(G.at[0, c], G.at[1 + d, c], gd_s.at[d], gd_r.at[d, c], tp=other).start()

    def stage_relay(c):
        for d, other in sides:
            arrived(G.at[1 + d, c], gd_r.at[d, c])
            half = pl.ds(d * H, H)
            remote(G.at[1 + d, c, half], G.at[3, c, half], gr_s.at[d], gr_r.at[d, c], tp=other).start()

    def stage_expert(c):
        @pl.when(c == 0)
        def _():
            for load in loads[9:]:
                load.wait()

        for d in range(2):
            arrived(G.at[3, c, pl.ds(d * H, H)], gr_r.at[d, c])
        owners = (y, down, up, far)
        total = jnp.zeros((S, 8, 1), F32)
        total_b = jnp.zeros((S, 8, 1), F32)
        for n in range(TP):
            g = G[n, c].astype(F32)
            a, b = g[:, :, :DS], g[:, :, DS:]
            total = total + jnp.sum(a * a, axis=2, keepdims=True)
            total_b = total_b + jnp.sum(b * b, axis=2, keepdims=True)
        width = DS * TP
        total_b = total_b + pltpu.roll(total_b, 4, axis=1)
        sa = lax.rsqrt(total / width + 1e-06)
        sb = lax.rsqrt(total_b / width + 1e-06)
        for n, owner in enumerate(owners):
            g = G[n, c].astype(F32)
            gn = gain[owner]
            nrm[owner, pl.ds(0, ar), :] = (g[:, :, :DS] * sa).reshape(ar, DS).astype(F32) * gn
            v0, v1 = from_message(g[:, :, DS:] * sb, S)
            nrm[owner, pl.ds(ar, rows - ar), pl.ds(0, h)] = v0 * gn[:, :h]
            nrm[owner, pl.ds(ar, rows - ar), pl.ds(h, h)] = v1 * gn[:, h:]
        lhs = jnp.concatenate([nrm[n].astype(BF) for n in range(TP)], axis=1)
        gate = jnp.dot(lhs, wg_v[...], preferred_element_type=F32)
        upper = jnp.dot(lhs, wu_v[...], preferred_element_type=F32)
        hidden = (gate / (1.0 + jnp.exp(-gate)) * upper).astype(BF)
        for q in range(TP):
            part = jnp.dot(hidden, wd_v[:, q * DS : (q + 1) * DS], preferred_element_type=F32)
            PS[c, q, :, :, pl.ds(0, DS)] = part[:ar].reshape(S, 8, DS).astype(BF)
            even, odd = to_message(part[ar:], S)
            for p in range(H):
                PS[c, q, 2 * p, :, pl.ds(DS, h)] = even[p].astype(BF)
                PS[c, q, 2 * p + 1, :, pl.ds(DS, h)] = odd[p].astype(BF)
        for d, other in sides:
            half, rest = pl.ds(d * H, H), pl.ds((1 - d) * H, H)
            remote(PS.at[c, far, half], R1.at[d, c], r1_s.at[d], r1_r.at[d, c], tp=other).start()
            remote(PS.at[c, other, rest], FR.at[d, c, rest], fi_s.at[d], fi_r.at[d, c], tp=other).start()

    def stage_add(c):
        for d, other in sides:
            half = pl.ds(d * H, H)
            arrived(R1.at[d, c], r1_r.at[d, c])
            ACC[d, c] = (PS[c, other, half].astype(F32) + R1[d, c].astype(F32)).astype(BF)
            remote(ACC.at[d, c], FR.at[d, c, half], fa_s.at[d], fa_r.at[d, c], tp=other).start()

    def stage_back(c):
        for d in range(2):
            arrived(FR.at[d, c, pl.ds((1 - d) * H, H)], fi_r.at[d, c])
            arrived(FR.at[d, c, pl.ds(d * H, H)], fa_r.at[d, c])
        whole = PS[c, y].astype(F32) + FR[0, c].astype(F32) + FR[1, c].astype(F32)
        FIN[c] = whole.astype(BF)

        @pl.when(c == 0)
        def _():
            ret[0, 0] = FIN[0, 0]

        plane = (taken >> (4 * c)) & 15
        dz = (iz - plane) & (NZ - 1)
        for r in range(S):
            send = remote(
                FIN.at[c, r], ret.at[dz, r], back_s, back_r.at[dz], ep=device(NZ - dz, NX - r // 2, r % 2)
            )
            if r:
                send.start()
            else:
                pl.when(c > 0)(send.start)

    @pl.loop(-3, NZ + 2)
    def _(u):
        @pl.when((u >= -1) & (u < NZ - 1))
        def _():
            stage_relay(u + 1)

        @pl.when(u < NZ - 3)
        def _():
            stage_direct(u + 3)

        if NZ > 6:
            pl.when(u == -3)(lambda: reach(3))

        @pl.when((u >= 0) & (u < NZ))
        def _():
            stage_expert(u)

        @pl.when((u >= 1) & (u < NZ + 1))
        def _():
            stage_add(u - 1)

        @pl.when(u == NZ)
        def _():
            pass_on(MS, MR1, MF, MACC, groups, m_sems)

            @pl.when(ic == 1)
            def _():
                pass_on(XS, XR1, XF, XACC, 2 * more, x_sems)

        @pl.when(u >= 2)
        def _():
            stage_back(u - 2)

    kept = groups * 8
    mixed[pl.ds(0, kept), :] = summed(MS, MF, groups, m_sems).reshape(kept, -1)
    result = remote(XO.at[0], XO.at[1], xo_s, xo_r, ep=buddy)

    @pl.when(ic == 1)
    def _():
        both = summed(XS, XF, 2 * more, x_sems)
        XO[0] = both[more:]
        result.start()
        mixed[pl.ds(kept, mrows - kept), :] = both[:more].reshape(mrows - kept, -1)

    @pl.when(ic == 0)
    def _():
        result.wait_recv()
        mixed[pl.ds(kept, mrows - kept), :] = XO[1].reshape(mrows - kept, -1)

    arrived(ret.at[0, pl.ds(1, S - 1)], back_r.at[0])
    for c in range(1, NZ):
        arrived(ret.at[c], back_r.at[c])
    back = ret[...].reshape(n_ep, 8, DS + h)
    ra = back[:, :, :DS].reshape(n_ep * 8, DS)
    b0, b1 = from_message(back[:, :, DS:].astype(F32), n_ep)
    rb = jnp.concatenate([b0, b1], axis=1).astype(BF)
    total = jnp.zeros((ntok, DS), F32)
    for q in range(2):
        row = jnp.dot(pick_a[q], ra, preferred_element_type=F32)
        row = row + jnp.dot(pick_b[q], rb, preferred_element_type=F32)
        total = total + row * share[q]
    routed[...] = total.astype(BF)

    for tail in tails:
        tail.wait_send()
    left(out.at[pl.ds(1, n_ep - 1)], disp_s)
    left(out.at[pl.ds(1, n_ep - 1)], back_s)
    for d in range(2):
        left(G.at[0], gd_s.at[d])
        left(R1.at[0], gr_s.at[d])
        left(R1.at[0], r1_s.at[d])
        left(R1.at[0], fi_s.at[d])
        left(R1.at[0], fa_s.at[d])
        left(MR1.at[0], m1_s.at[d])
        left(MR1.at[0], mi_s.at[d])
        left(MR1.at[0], ma_s.at[d])

    @pl.when(ic == 1)
    def _():
        result.wait_send()
        for d in range(2):
            left(XR1.at[0], x1_s.at[d])
            left(XR1.at[0], xi_s.at[d])
            left(XR1.at[0], xa_s.at[d])

    @pl.when(ic == 0)
    def _():
        for hand in handed:
            hand.wait_send()


def write_out(mixed, routed, mixed_out, routed_out, sems):
    copies = [
        pltpu.make_async_copy(mixed, mixed_out, sems.at[0]),
        pltpu.make_async_copy(routed, routed_out, sems.at[1]),
    ]
    for copy in copies:
        copy.start()
    for copy in copies:
        copy.wait()


def body(mix_bgate, mix_cgate, mix_input, conv_taps, mix_out_w, moe_x, moe_gain, routes, route_w, w_gate, w_up, w_down, *, dims):
    NZ, NX, _ = dims
    S = NX * 2
    H = S // 2
    n_ep = NZ * S
    ntok, DS = moe_x.shape
    D = DS * TP
    F = w_gate.shape[2]
    CH = mix_out_w.shape[0]
    ML = DS + DS // 2
    length = mix_input.shape[0]
    mrows = length // TP
    more = mrows // 16
    groups = mrows // 8 - more
    vmem = pl.BlockSpec(memory_space=pltpu.VMEM)
    hbm = pl.BlockSpec(memory_space=pltpu.HBM)
    V = pltpu.VMEM
    dma = pltpu.SemaphoreType.DMA
    results = pl.pallas_call(
        functools.partial(kernel, dims),
        name="step",
        out_shape=(
            V((mrows, D), BF),
            V((ntok, DS), BF),
        ),
        in_specs=[hbm] * 12,
        out_specs=(vmem, vmem),
        scratch_shapes=[
            V((length, CH), BF), V((length, CH), BF), V((length, CH), BF), V((3, CH), F32),
            V((ntok, DS), BF), V((TP, 1, DS), F32), V((2, ntok), jnp.int32), V((2, ntok), F32),
            V((D, F), BF), V((D, F), BF), V((F, D), BF), V((CH, D), BF),
            V((n_ep, 8, ML), BF),
            V((4, NZ, S, 8, ML), BF),
            V((TP, S * CAP, DS), F32),
            V((NZ, TP, S, 8, ML), BF),
            V((2, NZ, H, 8, ML), BF),
            V((2, NZ, S, 8, ML), BF),
            V((2, NZ, H, 8, ML), BF),
            V((NZ, S, 8, ML), BF),
            V((NZ, S, 8, ML), BF),
            V((2, 8, CH), BF),
            V((TP, groups, 8, D), BF),
            V((2, groups // 2, 8, D), BF),
            V((2, groups, 8, D), BF),
            V((2, groups // 2, 8, D), BF),
            V((TP, 2 * more, 8, D), BF),
            V((2, more, 8, D), BF),
            V((2, 2 * more, 8, D), BF),
            V((2, more, 8, D), BF),
            V((2, more, 8, D), BF),
            V((2, ntok, n_ep * 8), BF), V((2, ntok, n_ep * 4), BF),
            dma((12,)), dma((2,)), dma((2,)),
            dma, dma((NZ,)),
            dma((2,)), dma((2, NZ)), dma((2,)), dma((2, NZ)),
            dma((2,)), dma((2, NZ)), dma((2,)), dma((2, NZ)), dma((2,)), dma((2, NZ)),
            dma, dma((NZ,)),
            dma((2,)), dma((2,)), dma((2,)), dma((2,)), dma((2,)), dma((2,)),
            dma((2,)), dma((2,)), dma((2,)), dma((2,)), dma((2,)), dma((2,)),
            dma((TP,)), dma((TP,)), dma, dma, pltpu.SemaphoreType.REGULAR((NZ // 2, 2)),
        ],
        compiler_params=pltpu.CompilerParams(
            collective_id=0, has_side_effects=True, vmem_limit_bytes=67043328 - 2 * 2 * mrows * D - 16384
        ),
    )(
        mix_bgate, mix_cgate, mix_input, conv_taps, mix_out_w, moe_x,
        moe_gain.reshape(TP, 1, DS), routes.T, route_w.T, w_gate, w_up, w_down,
    )
    return pl.pallas_call(
        write_out,
        name="write_out",
        out_shape=tuple(jax.ShapeDtypeStruct(r.shape, BF) for r in results),
        in_specs=[vmem, vmem],
        out_specs=(hbm, hbm),
        scratch_shapes=[dma((2,))],
        compiler_params=pltpu.CompilerParams(vmem_limit_bytes=1024 * 1024),
    )(*results)


def solution(mesh):
    n_ep = mesh.shape["ep"]
    NZ, NX = (8, n_ep // 16) if n_ep >= 32 else (2, n_ep // 4)
    if NZ == 8:
        orders = (
            (0, 1, 2, 3, 4, 5, 6, 7),
            (1, 0, 2, 3, 5, 6, 4, 7),
            (2, 1, 3, 0, 6, 7, 5, 4),
            (3, 2, 1, 0, 7, 6, 5, 4),
            (4, 3, 2, 1, 0, 7, 6, 5),
            (5, 4, 3, 0, 1, 2, 7, 6),
            (6, 7, 0, 1, 2, 3, 4, 5),
            (7, 0, 1, 2, 3, 4, 5, 6),
        )
    else:
        orders = tuple(tuple((n + c) % NZ for c in range(NZ)) for n in range(NZ))
    in_specs = (
        P("ep", "tp"), P("ep", "tp"), P("ep", "tp"), P(None, "tp"), P("tp", None), P("ep", "tp"), P(),
        P("ep", None), P("ep", None), P("ep", None, "tp"), P("ep", None, "tp"), P("ep", "tp", None),
    )
    out_specs = (P(("ep", "tp"), None), P("ep", "tp"))
    return jax.shard_map(
        functools.partial(body, dims=(NZ, NX, orders)),
        mesh=mesh, in_specs=in_specs, out_specs=out_specs, check_vma=False,
    )
```
